256 devices in a mesh: sp: 32 (over z, x), tp: 8 (over y, core).
Axes of the slice: x: 4, y: 4, z: 8, core: 2. Of those that a mesh axis runs over, the one named last changes fastest.
Arguments:
- hidden_in: bfloat16 [12288, 2048], P('sp', 'tp'), may hold values from -6 to 6
- in_gain: float32 [2048], replicated, may hold values from 0.1 to 1.9
- receptance_weight: bfloat16 [2048, 1024], P(None, 'tp'), may hold values from -0.125 to 0.125
- key_weight: bfloat16 [2048, 1024], P(None, 'tp'), may hold values from -0.125 to 0.125
- value_weight: bfloat16 [2048, 1024], P(None, 'tp'), may hold values from -0.125 to 0.125
- decay_down: bfloat16 [2048, 128], replicated, may hold values from -0.125 to 0.125
- decay_up: bfloat16 [128, 1024], P(None, 'tp'), may hold values from -0.5 to 0.5
- decay_base: float32 [1024], P('tp'), may hold values from -14 to -2
- decay_shift: float32 [12288, 1024], P('sp', 'tp'), may hold values from -1 to 0
- learn_rate: float32 [1024], P('tp'), may hold values from 0 to 1
- query_pair: bfloat16 [2048, 8, 128], P(None, 'tp'), may hold values from -1 to 1
- key_pair: bfloat16 [2048, 8, 128], P(None, 'tp'), may hold values from -1 to 1
- value_pair: bfloat16 [2048, 8, 128], P(None, 'tp'), may hold values from -0.125 to 0.125
- mix_lambda: float32 [8], P('tp'), may hold values from 0.3 to 0.8
- out_recurrent: bfloat16 [1024, 2048], P('tp'), may hold values from -0.1875 to 0.1875
- out_attention: bfloat16 [1024, 2048], P('tp'), may hold values from -0.1875 to 0.1875
- out_gain: float32 [2048], replicated, may hold values from 0.1 to 1.9
Outputs:
- layer_out: bfloat16 [12288, 2048], P(('sp', 'tp'))
- log_sums: float32 [8, 2, 12288], P('tp', None, 'sp')
The draws below stay inside these ranges and needn't reach their ends.
All inputs are finite; a program needn't handle non-finite values.
Results may differ from the reference program's by a relative error of at most 0.018.
Values may be sent and summed in bfloat16 or wider, within the bound.
No kernel may reach another device: no remote copies, remote signals or barrier semaphores. Data moves between devices by JAX's collectives and lax.ppermute only.
A program may use at most 128 MiB of HBM per device.

```python
import math
import jax
import jax.numpy as jnp
from jax import lax

D = 2048
RH = 16
DH = 8
HD = 64
LOW = 128
TOK_DEV = 384
TOKENS = 12288
RD = 1024
DW = 1024


def paired_maps(key):
    base = jax.random.fold_in(key, 101)
    leading = jax.random.normal(jax.random.fold_in(base, 1), (D, DH, 2 * HD), jnp.float32) * (3.0 / D) ** 0.5
    trailing = jax.random.normal(jax.random.fold_in(base, 2), (D, DH, 2 * HD), jnp.float32) * D ** (-0.5)
    return (jnp.clip(leading, -1.0, 1.0), jnp.clip(trailing, -1.0, 1.0))


def draw_query_pair(key, part):
    return paired_maps(key)[0].astype(jnp.bfloat16)


def draw_key_pair(key, part):
    return paired_maps(key)[1].astype(jnp.bfloat16)


def draw_hidden_in(key, part):
    rows = jax.random.normal(jax.random.fold_in(key, 7), (TOKENS, D), jnp.float32)
    return jnp.clip(rows, -6.0, 6.0).astype(jnp.bfloat16)


def draw_decay_base(key, part):
    base = jax.random.fold_in(key, 23)
    share = 0.5
    slow = jax.random.uniform(jax.random.fold_in(base, 1), (RH, 1), jnp.float32) < share
    slow_level = jnp.log(jax.random.uniform(jax.random.fold_in(base, 2), (RH, HD), jnp.float32, 0.05, 0.25) / TOKENS)
    fast_level = jax.random.uniform(jax.random.fold_in(base, 3), (RH, HD), jnp.float32, -3.5, -2.0)
    return jnp.where(slow, slow_level, fast_level).reshape(RH * HD)


def draw_decay_shift(key, part):
    base = jax.random.fold_in(key, 31)
    block_total = TOKENS // TOK_DEV
    rates = jnp.exp(jax.random.uniform(jax.random.fold_in(base, 1), (block_total, 1, 1), jnp.float32, math.log(0.1), math.log(0.4))) / TOKENS
    steady = jnp.broadcast_to(rates, (block_total, TOK_DEV, RH * HD)).reshape(TOKENS, RH * HD)
    places = jax.random.randint(jax.random.fold_in(base, 2), (3,), 0, TOKENS)
    sizes = jax.random.uniform(jax.random.fold_in(base, 3), (3, RH * HD), jnp.float32, 0.22, 0.3)
    hits = (jnp.arange(TOKENS)[:, None] == places[None, :]).astype(jnp.float32)
    return -(steady + jnp.dot(hits, sizes))


def draw_learn_rate(key, part):
    base = jax.random.fold_in(key, 41)
    weak_level = jax.random.uniform(jax.random.fold_in(base, 1), (RH * HD,), jnp.float32, math.log(4.0), math.log(40.0))
    weak = jnp.exp(weak_level) / TOKENS
    strong = jnp.exp(jax.random.uniform(jax.random.fold_in(base, 2), (RH * HD,), jnp.float32, math.log(0.05), math.log(0.8)))
    picked = jax.random.randint(jax.random.fold_in(base, 3), (RH * HD,), 0, 8) < 5
    return jnp.where(picked, strong, weak)


def block_levels(rng, dims, shards, smallest, top_value):
    def one(position, blocks):
        heights = jax.random.uniform(jax.random.fold_in(jax.random.fold_in(rng, 6), position), (blocks,), jnp.float32, smallest / len(shards), top_value / len(shards))
        return jnp.repeat(jnp.exp(heights), dims[position] // blocks).reshape((-1,) + (1,) * (len(dims) - position - 1))

    level = one(*shards[0])
    for cut in shards[1:]:
        level = level * one(*cut)
    return level


def bell_draw(key, dims, scale, reach, pieces=(), held_as=jnp.bfloat16):
    values = scale * jax.random.normal(key, dims, jnp.float32)
    if pieces:
        values = values * block_levels(key, dims, pieces, -0.22, 0.18)
    return jnp.clip(values, -reach, reach).astype(held_as)


def setup_inputs(seed: int = 0) -> dict:
    key_list = jax.random.split(jax.random.key(seed), 18)
    return {
        "hidden_in": draw_hidden_in(jax.random.fold_in(key_list[17], 71), 0),
        "in_gain": jnp.clip(1.0 + 0.18 * jax.random.normal(key_list[1], (D,), jnp.float32), 0.1, 1.9),
        "receptance_weight": bell_draw(key_list[2], (D, RD), D ** -0.5, 0.125, ((1, 8),)),
        "key_weight": bell_draw(key_list[3], (D, RD), D ** -0.5, 0.125, ((1, 8),)),
        "value_weight": bell_draw(key_list[4], (D, RD), D ** -0.5, 0.125, ((1, 8),)),
        "decay_down": bell_draw(key_list[5], (D, LOW), D ** -0.5, 0.125),
        "decay_up": bell_draw(key_list[6], (LOW, RD), LOW ** -0.5, 0.5, ((1, 8),)),
        "decay_base": draw_decay_base(jax.random.fold_in(key_list[17], 71), 0),
        "decay_shift": draw_decay_shift(jax.random.fold_in(key_list[17], 71), 0),
        "learn_rate": draw_learn_rate(jax.random.fold_in(key_list[17], 71), 0),
        "query_pair": draw_query_pair(jax.random.fold_in(key_list[17], 71), 0),
        "key_pair": draw_key_pair(jax.random.fold_in(key_list[17], 71), 0),
        "value_pair": bell_draw(key_list[12], (D, DH, 2 * HD), D ** -0.5, 0.125, ((1, 8),)),
        "mix_lambda": jnp.clip(0.3 + 0.5 * jax.random.uniform(key_list[13], (DH,), jnp.float32) ** block_levels(key_list[13], (DH,), ((0, 8),), -0.2, 0.2), 0.3, 0.8),
        "out_recurrent": bell_draw(key_list[14], (RD, D), RD ** -0.5, 0.1875, ((0, 8),)),
        "out_attention": bell_draw(key_list[15], (DW, D), DW ** -0.5, 0.1875, ((0, 8),)),
        "out_gain": jnp.clip(1.0 + 0.18 * jax.random.normal(key_list[16], (D,), jnp.float32), 0.1, 1.9),
    }


HIGHEST = lax.Precision.HIGHEST
DECAY_SCALE = math.exp(-0.5)
NORM_EPS = 1e-06
GROUP_EPS = 0.00064
HEAD_EPS = 1e-05
KEY_EPS = 1e-06

def rms_rows(values, gain):
    wide = values.astype(jnp.float32)
    return wide * lax.rsqrt(lax.optimization_barrier(jnp.mean(wide * wide, axis=-1, keepdims=True)) + NORM_EPS) * gain

def project(normed, weight):
    return jnp.dot(normed, weight.reshape(D, -1), preferred_element_type=jnp.float32).astype(jnp.bfloat16)

def recurrence(receptance, key_rows, value_rows, log_decay, learn_rate):
    shape = (TOKENS, RH, HD)
    receptance = receptance.astype(jnp.float32).reshape(shape)
    key_rows = key_rows.astype(jnp.float32).reshape(shape)
    value_rows = value_rows.astype(jnp.float32).reshape(shape)
    decay = jnp.exp(log_decay).reshape(shape)
    unit_keys = key_rows * lax.rsqrt(lax.optimization_barrier(jnp.sum(key_rows * key_rows, axis=-1, keepdims=True)) + KEY_EPS)
    erasing = unit_keys * learn_rate.reshape(RH, HD)

    def advance(carried, inputs):
        read_now, decay_now, key_now, value_now, unit_now, erase_now = inputs
        removed = jnp.einsum('hvk,hk->hv', carried, unit_now, precision=HIGHEST)
        carried = carried * decay_now[:, None, :] - removed[:, :, None] * erase_now[:, None, :] + value_now[:, :, None] * key_now[:, None, :]
        return (carried, jnp.einsum('hvk,hk->hv', carried, read_now, precision=HIGHEST))
    initial = jnp.zeros((RH, HD, HD), jnp.float32)
    outputs = lax.scan(advance, initial, (receptance, decay, key_rows, value_rows, unit_keys, erasing))[1]
    centered = outputs - lax.optimization_barrier(jnp.mean(outputs, axis=-1, keepdims=True))
    normal = centered * lax.rsqrt(lax.optimization_barrier(jnp.mean(centered * centered, axis=-1, keepdims=True)) + GROUP_EPS)
    return normal.reshape(TOKENS, RH * HD).astype(jnp.bfloat16)

def differential(queries, pair_keys, pair_values, mix_lambda):
    places = jnp.arange(TOKENS)
    score_scale = HD ** (-0.5)
    block_count = TOKENS // TOK_DEV

    def one_head(inputs):
        head_queries, head_keys, head_values, head_lambda = inputs
        keys_wide = head_keys.astype(jnp.float32).reshape(TOKENS, 2, HD)
        values_wide = head_values.astype(jnp.float32)
        query_blocks = head_queries.reshape(block_count, TOK_DEV, 2, HD)

        def one_block(block_inputs):
            block_queries, block_number = block_inputs
            rows_at = block_number * TOK_DEV + jnp.arange(TOK_DEV)
            scores = jnp.einsum('qmd,kmd->mqk', block_queries.astype(jnp.float32), keys_wide) * score_scale
            allowed = rows_at[:, None] >= places[None, :]
            scores = jnp.where(allowed[None], scores, -jnp.inf)
            row_max = lax.optimization_barrier(jnp.max(scores, axis=-1, keepdims=True))
            weights = jnp.exp(scores - row_max)
            row_sum = lax.optimization_barrier(jnp.sum(weights, axis=-1, keepdims=True))
            rounded = lax.optimization_barrier(weights.astype(jnp.bfloat16)).astype(jnp.float32)
            map_out = jnp.einsum('mqk,kv->mqv', rounded, values_wide) / row_sum
            head_out = map_out[0] - head_lambda * map_out[1]
            head_out = head_out * lax.rsqrt(lax.optimization_barrier(jnp.mean(head_out * head_out, axis=-1, keepdims=True)) + HEAD_EPS)
            return (head_out, (row_max + jnp.log(row_sum))[..., 0])
        outs, sums = lax.map(one_block, (query_blocks, jnp.arange(block_count)))
        return (outs.reshape(TOKENS, 2 * HD), sums.transpose(1, 0, 2).reshape(2, TOKENS))
    head_outs, log_sums = lax.map(one_head, (queries.transpose(1, 0, 2), pair_keys.transpose(1, 0, 2), pair_values.transpose(1, 0, 2), mix_lambda))
    att_mix = head_outs.transpose(1, 0, 2).reshape(TOKENS, DH * 2 * HD).astype(jnp.bfloat16)
    return (att_mix, log_sums)

def reference(hidden_in, in_gain, receptance_weight, key_weight, value_weight, decay_down, decay_up, decay_base, decay_shift, learn_rate, query_pair, key_pair, value_pair, mix_lambda, out_recurrent, out_attention, out_gain):
    normed = rms_rows(hidden_in, in_gain).astype(jnp.bfloat16)
    receptance = project(normed, receptance_weight)
    rec_keys = project(normed, key_weight)
    rec_values = project(normed, value_weight)
    low_rank = jnp.tanh(jnp.dot(normed, decay_down, preferred_element_type=jnp.float32)).astype(jnp.bfloat16)
    log_decay = -DECAY_SCALE * jax.nn.sigmoid(jnp.dot(low_rank, decay_up, preferred_element_type=jnp.float32) + decay_base) + decay_shift
    rec_mix = recurrence(receptance, rec_keys, rec_values, log_decay, learn_rate)
    queries = project(normed, query_pair).reshape(TOKENS, DH, 2 * HD)
    pair_keys = project(normed, key_pair).reshape(TOKENS, DH, 2 * HD)
    pair_values = project(normed, value_pair).reshape(TOKENS, DH, 2 * HD)
    att_mix, log_sums = differential(queries, pair_keys, pair_values, mix_lambda)
    projected = jnp.dot(rec_mix, out_recurrent, preferred_element_type=jnp.float32) + jnp.dot(att_mix, out_attention, preferred_element_type=jnp.float32)
    return (rms_rows(projected, out_gain).astype(jnp.bfloat16), log_sums)
```

```python
import functools
import math

import jax
import jax.numpy as jnp
from jax import lax
from jax.experimental import pallas as pl
from jax.experimental.pallas import tpu as pltpu
from jax.sharding import Mesh
from jax.sharding import PartitionSpec as P

HD = 64
F32 = jnp.float32
BF16 = jnp.bfloat16
HIGHEST = lax.Precision.HIGHEST
DECAY_SCALE = math.exp(-0.5)
NORM_EPS = 1e-06
GROUP_EPS = 0.00064
HEAD_EPS = 1e-05
KEY_EPS = 1e-06
NEGATIVE = -1e30
SPAN = 64
VMEM_LIMIT = 60 * 1024 * 1024
NT = (((1,), (1,)), ((), ()))
TN = (((0,), (0,)), ((), ()))
NN = (((1,), (0,)), ((), ()))


def whole(shape_like):
    return pl.BlockSpec(memory_space=pltpu.VMEM)


def call(kernel, outs, scalars, arrays, scratch=(), flops=0, name=None):
    return pl.pallas_call(
        kernel,
        out_shape=outs,
        in_specs=[pl.BlockSpec(memory_space=pltpu.SMEM)] * len(scalars)
        + [pl.BlockSpec(memory_space=pltpu.VMEM)] * len(arrays),
        out_specs=jax.tree.map(lambda _: pl.BlockSpec(memory_space=pltpu.VMEM), outs),
        scratch_shapes=list(scratch),
        compiler_params=pltpu.CompilerParams(vmem_limit_bytes=VMEM_LIMIT),
        cost_estimate=pl.CostEstimate(flops=flops, bytes_accessed=flops // 1000, transcendentals=0),
        name=name,
    )(*scalars, *arrays)


def dot(left, right, dims=NN, precision=None):
    return lax.dot_general(left, right, dims, precision=precision, preferred_element_type=F32)


def exact(left, right, dims=NN):
    return dot(left, right, dims, HIGHEST)


def ring(size, shift):
    return [(i, (i + shift) % size) for i in range(size)]


def lane_ids(shape):
    return lax.broadcasted_iota(jnp.int32, shape, len(shape) - 1)


def row_ids(shape):
    return lax.broadcasted_iota(jnp.int32, shape, len(shape) - 2)


def project_kernel(
    piece_ref,
    h0, h1, h2, h3, h4, g0, g1, g2, g3, g4,
    gain_ref, wr, wk, wv, wd, wq, wkp, wvp, up_ref, base_ref, shift_ref,
    q_out, kv_out, r_out, k_out, v_out, decay_out,
    normed,
):
    pieces = []
    for own, up, down, far_a, far_b in ((h0, h1, h2, h3, h4), (g0, g1, g2, g3, g4)):
        pieces += [own[...], up[...], down[...], jnp.concatenate([far_a[...], far_b[...]], axis=0)]
    squares = None
    for piece in pieces:
        wide = piece.astype(F32)
        part = wide * wide
        part = part[:, :128] + part[:, 128:]
        squares = part if squares is None else squares + part
    scale = lax.rsqrt(jnp.sum(squares, axis=-1, keepdims=True) / 2048.0 + NORM_EPS)
    for number, piece in enumerate(pieces):
        place = piece_ref[number]
        gain = gain_ref[pl.ds(place, 1), :]
        value = (piece.astype(F32) * scale * gain).astype(BF16)
        normed[:, pl.ds(pl.multiple_of(place * 256, 256), 256)] = value

    def pair(first, second):
        return dot(normed[...], jnp.concatenate([first[...], second[...]], axis=1))

    kv_out[...] = pair(wkp, wvp).astype(BF16)
    both = pair(wd, wq)
    q_out[...] = both[:, 128:].astype(BF16)
    low = jnp.tanh(both[:, :128]).astype(BF16)
    pre = dot(low, up_ref[...]) + base_ref[...]
    decay_out[...] = -DECAY_SCALE * jax.nn.sigmoid(pre) + shift_ref[...]
    both = pair(wr, wk)
    r_out[...] = both[:, :128].astype(BF16)
    k_out[...] = both[:, 128:].astype(BF16)
    v_out[...] = dot(normed[...], wv[...]).astype(BF16)


def masks():
    rows, lanes = row_ids((128, 128)), lane_ids((128, 128))
    same = (rows < HD) == (lanes < HD)
    return same


def compose(earlier, later, same):
    return exact(earlier, jnp.where(same, later, 0.0)) + jnp.where(same, 0.0, later)


def recurrent_kernel(r_ref, k_ref, v_ref, decay_ref, rate_ref, q_out, local_out, total_out):
    rows = r_ref.shape[0]
    count = rows // SPAN
    same = masks()
    ones_block = jnp.where(same, 1.0, 0.0).astype(F32)
    diagonal = row_ids((128, 128)) == lane_ids((128, 128))
    first = lane_ids((SPAN, 128)) < HD
    t_ids = row_ids((SPAN, 128))
    s_ids = lane_ids((SPAN, 128)) % HD
    strict = s_ids < t_ids
    causal = s_ids <= t_ids
    tri = jnp.where(row_ids((SPAN, SPAN)) >= lane_ids((SPAN, SPAN)), 1.0, 0.0).astype(F32)
    keep = (first, jnp.logical_not(first))
    units, chunks = [], []
    for c in range(count):
        at = slice(c * SPAN, (c + 1) * SPAN)
        decay = decay_ref[at, :]
        running = exact(tri, decay)
        before = running - decay
        middle = running[SPAN // 2 - 1 : SPAN // 2, :]
        ending = running[SPAN - 1 : SPAN, :]
        keys = k_ref[at, :].astype(F32)
        reads = r_ref[at, :].astype(F32)
        values = v_ref[at, :].astype(F32)
        unit_keys = keys * lax.rsqrt(exact(keys * keys, ones_block) + KEY_EPS)
        erasing = unit_keys * rate_ref[...]
        grow = jnp.exp(middle - running)
        against = -unit_keys * jnp.exp(before - middle)
        read_scaled = reads * jnp.exp(running - middle)
        right = jnp.concatenate([erasing * grow, keys * grow], axis=0)
        zero = jnp.zeros((SPAN, 128), F32)
        left = jnp.concatenate(
            [jnp.where(k, side, 0.0) for k in keep for side in (against, read_scaled)], axis=0
        )
        scores = exact(left, right, NT)
        turned = pltpu.roll(values, HD, 1)
        to_end = jnp.exp(ending - running)
        ends = jnp.concatenate([erasing * to_end, keys * to_end], axis=0)
        start = -unit_keys * jnp.exp(before)
        chunks.append((reads * jnp.exp(running), ends, jnp.exp(ending)))
        for h in range(2):
            lower = jnp.where(strict, scores[128 * h : 128 * h + SPAN], 0.0)
            reading = jnp.where(causal, scores[128 * h + SPAN : 128 * h + 128], 0.0)
            side_values = jnp.where(keep[h], 0.0, turned)
            rhs = jnp.where(keep[h], start, 0.0) + exact(
                lower, jnp.concatenate([zero, side_values], axis=0)
            )
            units.append((lower, reading, side_values, rhs))
    solved = []
    group = 4
    for base in range(0, len(units), group):
        some = units[base : base + group]
        state = [[u[3][8 * b : 8 * b + 8] for b in range(SPAN // 8)] for u in some]
        for s in range(SPAN - 1):
            for n, u in enumerate(some):
                row = state[n][s // 8][s % 8 : s % 8 + 1]
                for b in range(s // 8 if s % 8 < 7 else s // 8 + 1, SPAN // 8):
                    state[n][b] = state[n][b] + u[0][8 * b : 8 * b + 8, s : s + 1] * row
        solved += [jnp.concatenate(one, axis=0) for one in state]
    prefix = jnp.where(diagonal, 1.0, 0.0).astype(F32)
    for c in range(count):
        decayed_reads, ends, last = chunks[c]
        got, moved = [], []
        for h in range(2):
            _, reading, side_values, _ = units[2 * c + h]
            both = jnp.concatenate([solved[2 * c + h], side_values], axis=0)
            got.append(exact(reading, both))
            moved.append(exact(both, ends, TN))
        lanes = lane_ids((128, 128)) < HD
        step = jnp.where(lanes, moved[0], moved[1]) + jnp.where(diagonal, last, 0.0)
        read_state = jnp.where(first, got[0], got[1]) + decayed_reads
        local = jnp.where(first, got[1], got[0])
        at = slice(c * SPAN, (c + 1) * SPAN)
        q_out[at, :] = exact(read_state, jnp.where(same, prefix, 0.0), NT)
        local_out[at, :] = local + exact(read_state, jnp.where(same, 0.0, prefix), NT)
        prefix = compose(prefix, step, same)
    total_out[...] = prefix.astype(BF16)


def along_x_kernel(place_ref, parts_ref, before_out, total_out):
    same = masks()
    identity = jnp.where(row_ids((128, 128)) == lane_ids((128, 128)), 1.0, 0.0).astype(F32)
    parts = [parts_ref[j].astype(F32) for j in range(4)]
    mine = place_ref[0]
    total_out[...] = compose(
        compose(parts[0], parts[1], same), compose(parts[2], parts[3], same), same
    ).astype(BF16)
    kept = [jnp.where(j < mine, parts[j], identity) for j in range(3)]
    before_out[...] = compose(compose(kept[0], kept[1], same), kept[2], same)


def along_z_kernel(place_ref, parts_ref, before_ref, state_out):
    same = masks()
    identity = jnp.where(row_ids((128, 128)) == lane_ids((128, 128)), 1.0, 0.0).astype(F32)
    mine = place_ref[0]
    level = [jnp.where(j < mine, parts_ref[j].astype(F32), identity) for j in range(7)]
    level.append(before_ref[...])
    while len(level) > 1:
        level = [compose(level[i], level[i + 1], same) for i in range(0, len(level), 2)]
    state_out[...] = jnp.where(same, 0.0, level[0])


def attention_kernel(
    place_ref, q0, q1, q2, q3, kv0, kv1, kv2, kv3, kv4, kv5, kv6, kv7a, kv7b,
    o0, o1, o2, o3,
    keys, values, row_max, weighted,
):
    rows = q0.shape[0]
    my_z, my_x = place_ref[0], place_ref[1]
    ones = jnp.ones((rows, 128), BF16)

    def place(block, at):
        keys[at] = block[:, :128]
        values[at] = jnp.concatenate([block[:, 128:], ones], axis=1)

    for number, ref in enumerate((kv0, kv1, kv2, kv3, kv4, kv5, kv6)):
        place(ref[...], place_ref[2 + number])
    place(jnp.concatenate([kv7a[...], kv7b[...]], axis=0), place_ref[9])
    first = lane_ids((rows, 128)) < HD

    def one_block(queries, at, diagonal):
        key_block, value_block = keys[at], values[at]
        for m in range(2):
            scores = dot(queries[m], key_block, NT)
            if diagonal:
                allowed = row_ids((rows, rows)) >= lane_ids((rows, rows))
                scores = jnp.where(allowed, scores, NEGATIVE)
            old = row_max[m]
            new = jnp.maximum(old, jnp.max(scores, axis=-1, keepdims=True))
            weights = jnp.exp(scores - new[:, :1]).astype(BF16)
            rescale = jnp.exp(old - new)
            row_max[m] = new
            weighted[m] = weighted[m] * jnp.concatenate([rescale, rescale], axis=1) + dot(
                weights, value_block
            )

    for number, (q_ref, out) in enumerate(((q0, o0), (q1, o1), (q2, o2), (q3, o3))):
        x_of = place_ref[10 + number]
        scaled = (q_ref[...].astype(F32) * (HD**-0.5)).astype(BF16)
        queries = [jnp.where(first, scaled, 0).astype(BF16), jnp.where(first, 0, scaled).astype(BF16)]
        row_max[...] = jnp.full_like(row_max, NEGATIVE)
        weighted[...] = jnp.zeros_like(weighted)

        def step(at, carry):
            one_block(queries, at, False)
            return carry

        lax.fori_loop(0, jnp.where(x_of > my_x, my_z + 1, my_z), step, 0)

        @pl.when(x_of == my_x)
        def _():
            one_block(queries, my_z, True)

        for m in range(2):
            row_sum = weighted[m][:, 128:]
            some = row_sum > 0.0
            safe = jnp.where(some, row_sum, 1.0)
            out[m, :rows, :] = (weighted[m][:, :128] / safe).astype(BF16)
            logs = jnp.where(some, row_max[m] + jnp.log(safe), NEGATIVE)
            line = jnp.transpose(logs)[:1, :]
            lines = [line[:, 128 * j : 128 * j + 128] for j in range(rows // 128)]
            high = [a.astype(BF16).astype(F32) for a in lines]
            middle = [(a - b).astype(BF16).astype(F32) for a, b in zip(lines, high)]
            low = [a - b - c for a, b, c in zip(lines, high, middle)]
            tail = high + middle + low
            tail += [jnp.zeros((16 - len(tail), 128), F32)]
            out[m, rows:, :] = jnp.concatenate(tail, axis=0).astype(BF16)


def finish_kernel(
    place_ref, lambda_ref, p0, p1, p2, p3, read_ref, local_ref, state_ref, wr_ref, wa_ref,
    mine_out, other_out, logs_out,
):
    rows = read_ref.shape[0]
    parts = (p0, p1, p2, p3)
    maps = []
    for m in range(2):
        logs = []
        for p in parts:
            tail = p[m, rows:, :].astype(F32)
            n = rows // 128
            logs.append(
                jnp.concatenate(
                    [tail[j : j + 1] + tail[n + j : n + j + 1] + tail[2 * n + j : 2 * n + j + 1] for j in range(n)],
                    axis=1,
                )
            )
        top = functools.reduce(jnp.maximum, logs)
        shares = [jnp.exp(a - top) for a in logs]
        total = functools.reduce(jnp.add, shares)
        logs_out[m : m + 1, :] = top + jnp.log(total)
        got = None
        for p, share in zip(parts, shares):
            column = jnp.transpose(jnp.broadcast_to(share / total, (128, rows)))
            term = p[m, :rows, :].astype(F32) * column
            got = term if got is None else got + term
        maps.append(got)
    head = maps[0] - lambda_ref[0] * maps[1]
    head = head * lax.rsqrt(jnp.mean(head * head, axis=-1, keepdims=True) + HEAD_EPS)
    att_mix = head.astype(BF16)
    recurrent = local_ref[...] + exact(read_ref[...], state_ref[...], NT)
    recurrent = pltpu.roll(recurrent, HD, 1)
    first = lane_ids((rows, 128)) < HD

    def per_head(values):
        low = jnp.sum(jnp.where(first, values, 0.0), axis=-1, keepdims=True)
        high = jnp.sum(jnp.where(first, 0.0, values), axis=-1, keepdims=True)
        return jnp.where(first, low, high) / HD

    centered = recurrent - per_head(recurrent)
    rec_mix = (centered * lax.rsqrt(per_head(centered * centered) + GROUP_EPS)).astype(BF16)
    mix = jnp.concatenate([rec_mix, att_mix], axis=1)
    core = place_ref[0]
    for n in range(8):
        at = slice(256 * n, 256 * n + 256)
        weight = jnp.concatenate([wr_ref[:, at], wa_ref[:, at]], axis=0)
        got = dot(mix, weight).astype(BF16)
        for y in range(4):
            even = got[96 * y : 96 * y + 48]
            odd = got[96 * y + 48 : 96 * y + 96]
            mine_out[y, :, at] = jnp.where(core == 0, even, odd)
            other_out[y, :, at] = jnp.where(core == 0, odd, even)


def rms_rows(values, gain):
    return values * lax.rsqrt(jnp.mean(values * values, axis=-1, keepdims=True) + NORM_EPS) * gain


def per_device(
    hidden_in, in_gain, receptance_weight, key_weight, value_weight, decay_down, decay_up,
    decay_base, decay_shift, learn_rate, query_pair, key_pair, value_pair, mix_lambda,
    out_recurrent, out_attention, out_gain,
):
    permute = lax.ppermute
    z, x, y, core = (lax.axis_index(a) for a in ("z", "x", "y", "c"))
    rows = hidden_in.shape[0]
    half = rows // 2
    shaped = jax.ShapeDtypeStruct

    up = permute(hidden_in, "y", ring(4, 1))
    down = permute(hidden_in, "y", ring(4, -1))
    far_a = permute(up[:half], "y", ring(4, 1))
    far_b = permute(down[half:], "y", ring(4, -1))
    mine = [hidden_in, up, down, far_a, far_b]
    theirs = [permute(a, "c", ring(2, 1)) for a in mine]
    ys = jnp.stack([y, (y + 3) % 4, (y + 1) % 4, (y + 2) % 4])
    piece_at = jnp.concatenate([ys * 2 + core, ys * 2 + 1 - core]).astype(jnp.int32)

    q, kv, r, k, v, decay = call(
        project_kernel,
        (
            shaped((rows, 128), BF16), shaped((rows, 256), BF16), shaped((rows, 128), BF16),
            shaped((rows, 128), BF16), shaped((rows, 128), BF16), shaped((rows, 128), F32),
        ),
        (piece_at,),
        (
            *mine, *theirs, in_gain.reshape(8, 256), receptance_weight, key_weight, value_weight,
            decay_down, query_pair.reshape(2048, 128), key_pair.reshape(2048, 128),
            value_pair.reshape(2048, 128), decay_up, decay_base.reshape(1, 128), decay_shift,
        ),
        scratch=(pltpu.VMEM((rows, 2048), BF16),),
        flops=2 * rows * 2048 * 896,
        name="project",
    )

    read, local, total = call(
        recurrent_kernel,
        (shaped((rows, 128), F32), shaped((rows, 128), F32), shaped((128, 128), BF16)),
        (),
        (r, k, v, decay, learn_rate.reshape(1, 128)),
        flops=10**9,
        name="recurrent",
    )
    parts = lax.all_to_all(
        jnp.broadcast_to(total, (4, 128, 128)), "x", 0, 0, tiled=True
    )
    before, line = call(
        along_x_kernel,
        (shaped((128, 128), F32), shaped((128, 128), BF16)),
        (x.reshape(1),), (parts,), flops=10**8, name="along_x",
    )
    parts = lax.all_to_all(jnp.broadcast_to(line, (8, 128, 128)), "z", 0, 0, tiled=True)
    state = call(
        along_z_kernel, shaped((128, 128), F32), (z.reshape(1),), (parts, before),
        flops=10**8, name="along_z",
    )

    q1 = permute(q, "x", ring(4, 1))
    q2 = permute(q, "x", ring(4, -1))
    q3 = permute(q, "x", ring(4, 2))
    top, bottom = kv[:half], kv[half:]
    kvs = [kv]
    right, left = (top, bottom), (top, bottom)
    for _ in range(3):
        right = tuple(permute(a, "z", ring(8, 1)) for a in right)
        left = tuple(permute(a, "z", ring(8, -1)) for a in left)
        kvs += [jnp.concatenate(right, axis=0), jnp.concatenate(left, axis=0)]
    last_top = permute(right[0], "z", ring(8, 1))
    last_bottom = permute(left[1], "z", ring(8, -1))
    places = jnp.stack(
        [z, x, z]
        + [a for s in (1, 2, 3) for a in ((z + 8 - s) % 8, (z + s) % 8)]
        + [(z + 4) % 8, x, (x + 3) % 4, (x + 1) % 4, (x + 2) % 4]
    ).astype(jnp.int32)
    payload = shaped((2, rows + 16, 128), BF16)
    outs = call(
        attention_kernel,
        (payload,) * 4,
        (places,),
        (q, q1, q2, q3, *kvs, last_top, last_bottom),
        scratch=(
            pltpu.VMEM((8, rows, 128), BF16), pltpu.VMEM((8, rows, 256), BF16),
            pltpu.VMEM((2, rows, 128), F32), pltpu.VMEM((2, rows, 256), F32),
        ),
        flops=8 * 10**9,
        name="attention",
    )
    back = [
        outs[0],
        permute(outs[1], "x", ring(4, -1)),
        permute(outs[2], "x", ring(4, 1)),
        permute(outs[3], "x", ring(4, 2)),
    ]
    ours, others, log_sums = call(
        finish_kernel,
        (shaped((4, rows // 8, 2048), BF16), shaped((4, rows // 8, 2048), BF16), shaped((2, rows), F32)),
        (core.reshape(1), mix_lambda),
        (*back, read, local, state, out_recurrent, out_attention),
        flops=10**9,
        name="finish",
    )
    theirs = permute(others, "c", ring(2, 1))
    summed = (ours.astype(F32) + theirs.astype(F32)).astype(BF16)
    parts = lax.all_to_all(summed, "y", 0, 0, tiled=True)
    projected = jnp.sum(parts.astype(F32), axis=0)
    layer_out = rms_rows(projected, out_gain).astype(BF16)
    return (layer_out, log_sums[None])


def solution(mesh):
    split = Mesh(mesh.devices.reshape(8, 4, 4, 2), ("z", "x", "y", "c"))
    sp, tp = ("z", "x"), ("y", "c")
    placed = (
        P(sp, tp), P(), P(None, tp), P(None, tp), P(None, tp), P(), P(None, tp), P(tp), P(sp, tp),
        P(tp), P(None, tp, None), P(None, tp, None), P(None, tp, None), P(tp), P(tp, None),
        P(tp, None), P(),
    )
    return jax.shard_map(
        per_device,
        mesh=split,
        in_specs=placed,
        out_specs=(P(("z", "x", "y", "c"), None), P(tp, None, sp)),
        check_vma=False,
    )
```

```python
import functools
import math

import jax
import jax.numpy as jnp
from jax import lax
from jax.experimental import pallas as pl
from jax.experimental.pallas import tpu as pltpu
from jax.sharding import Mesh
from jax.sharding import PartitionSpec as P

HD = 64
F32 = jnp.float32
BF16 = jnp.bfloat16
HIGHEST = lax.Precision.HIGHEST
DECAY_SCALE = math.exp(-0.5)
NORM_EPS = 1e-06
GROUP_EPS = 0.00064
HEAD_EPS = 1e-05
KEY_EPS = 1e-06
NEGATIVE = -1e30
SPAN = 64
VMEM_LIMIT = 60 * 1024 * 1024
NT = (((1,), (1,)), ((), ()))
TN = (((0,), (0,)), ((), ()))
NN = (((1,), (0,)), ((), ()))


def call(kernel, outs, scalars, arrays, scratch=(), flops=0, name=None):
    return pl.pallas_call(
        kernel,
        out_shape=outs,
        in_specs=[pl.BlockSpec(memory_space=pltpu.SMEM)] * len(scalars)
        + [pl.BlockSpec(memory_space=pltpu.VMEM)] * len(arrays),
        out_specs=jax.tree.map(lambda _: pl.BlockSpec(memory_space=pltpu.VMEM), outs),
        scratch_shapes=list(scratch),
        compiler_params=pltpu.CompilerParams(vmem_limit_bytes=VMEM_LIMIT),
        cost_estimate=pl.CostEstimate(flops=flops, bytes_accessed=flops // 1000, transcendentals=0),
        name=name,
    )(*scalars, *arrays)


def dot(left, right, dims=NN, precision=None):
    return lax.dot_general(left, right, dims, precision=precision, preferred_element_type=F32)


def exact(left, right, dims=NN):
    return dot(left, right, dims, HIGHEST)


def ring(size, shift):
    return [(i, (i + shift) % size) for i in range(size)]


def lane_ids(shape):
    return lax.broadcasted_iota(jnp.int32, shape, len(shape) - 1)


def row_ids(shape):
    return lax.broadcasted_iota(jnp.int32, shape, len(shape) - 2)


def project_kernel(
    piece_ref,
    h0, h1, h2, h3, h4, g0, g1, g2, g3, g4,
    gain_ref, wq, wkp, wvp,
    normed, q_out, kv_out,
):
    pieces = []
    for own, up, down, far_a, far_b in ((h0, h1, h2, h3, h4), (g0, g1, g2, g3, g4)):
        pieces += [own[...], up[...], down[...], jnp.concatenate([far_a[...], far_b[...]], axis=0)]
    squares = None
    for piece in pieces:
        wide = piece.astype(F32)
        part = wide * wide
        part = part[:, :128] + part[:, 128:]
        squares = part if squares is None else squares + part
    scale = lax.rsqrt(jnp.sum(squares, axis=-1, keepdims=True) / 2048.0 + NORM_EPS)
    for number, piece in enumerate(pieces):
        place = piece_ref[number]
        gain = gain_ref[pl.ds(place, 1), :]
        value = (piece.astype(F32) * scale * gain).astype(BF16)
        normed[:, pl.ds(pl.multiple_of(place * 256, 256), 256)] = value
    kv_out[...] = dot(normed[...], jnp.concatenate([wkp[...], wvp[...]], axis=1)).astype(BF16)
    q_out[...] = dot(normed[...], wq[...]).astype(BF16)


def same_head():
    return (row_ids((128, 128)) < HD) == (lane_ids((128, 128)) < HD)


def diagonal_mask():
    return row_ids((128, 128)) == lane_ids((128, 128))


def compose(earlier, later, same):
    return exact(earlier, jnp.where(same, later, 0.0)) + jnp.where(same, 0.0, later)


def chunk_kernel(
    normed, wr, wk, wv, wd, up_ref, base_ref, shift_ref, rate_ref,
    lower_out, reading_out, rhs_out, turned_out, reads_out, ends_out, last_out,
):
    both = dot(normed[...], jnp.concatenate([wr[...], wk[...]], axis=1))
    all_reads = both[:, :128].astype(BF16)
    all_keys = both[:, 128:].astype(BF16)
    both = dot(normed[...], jnp.concatenate([wv[...], wd[...]], axis=1))
    all_values = both[:, :128].astype(BF16)
    low = jnp.tanh(both[:, 128:]).astype(BF16)
    pre = dot(low, up_ref[...]) + base_ref[...]
    all_decay = -DECAY_SCALE * jax.nn.sigmoid(pre) + shift_ref[...]
    rows = normed.shape[0]
    count = rows // SPAN
    ones_block = jnp.where(same_head(), 1.0, 0.0).astype(F32)
    first = lane_ids((SPAN, 128)) < HD
    t_ids = row_ids((SPAN, 128))
    s_ids = lane_ids((SPAN, 128)) % HD
    strict = s_ids < t_ids
    causal = s_ids <= t_ids
    tri = jnp.where(row_ids((SPAN, SPAN)) >= lane_ids((SPAN, SPAN)), 1.0, 0.0).astype(F32)
    keep = (first, jnp.logical_not(first))
    zero = jnp.zeros((SPAN, 128), F32)
    for c in range(count):
        at = slice(c * SPAN, (c + 1) * SPAN)
        decay = all_decay[at, :]
        running = exact(tri, decay)
        before = running - decay
        middle = running[SPAN // 2 - 1 : SPAN // 2, :]
        ending = running[SPAN - 1 : SPAN, :]
        keys = all_keys[at, :].astype(F32)
        reads = all_reads[at, :].astype(F32)
        values = all_values[at, :].astype(F32)
        unit_keys = keys * lax.rsqrt(exact(keys * keys, ones_block) + KEY_EPS)
        erasing = unit_keys * rate_ref[...]
        grow = jnp.exp(middle - running)
        against = -unit_keys * jnp.exp(before - middle)
        read_scaled = reads * jnp.exp(running - middle)
        right = jnp.concatenate([erasing * grow, keys * grow], axis=0)
        left = jnp.concatenate(
            [jnp.where(k, side, 0.0) for k in keep for side in (against, read_scaled)], axis=0
        )
        scores = exact(left, right, NT)
        turned = pltpu.roll(values, HD, 1)
        to_end = jnp.exp(ending - running)
        ends_out[c] = jnp.concatenate([erasing * to_end, keys * to_end], axis=0)
        start = -unit_keys * jnp.exp(before)
        reads_out[c] = reads * jnp.exp(running)
        last_out[c] = jnp.broadcast_to(jnp.exp(ending), (8, 128))
        turned_out[c] = turned
        for h in range(2):
            lower = jnp.where(strict, scores[128 * h : 128 * h + SPAN], 0.0)
            lower_out[2 * c + h] = lower
            reading_out[2 * c + h] = jnp.where(causal, scores[128 * h + SPAN : 128 * h + 128], 0.0)
            side_values = jnp.where(keep[h], 0.0, turned)
            rhs_out[2 * c + h] = jnp.where(keep[h], start, 0.0) + exact(
                lower, jnp.concatenate([zero, side_values], axis=0)
            )


def recurrent_kernel(
    lower_ref, reading_ref, rhs_ref, turned_ref, reads_ref, ends_ref, last_ref, query_ref,
    read_out, local_out, message_out,
):
    count = turned_ref.shape[0]
    rows = count * SPAN
    same = same_head()
    diagonal = diagonal_mask()
    first = lane_ids((SPAN, 128)) < HD
    keep = (first, jnp.logical_not(first))
    solved = []
    group = 4
    for base in range(0, 2 * count, group):
        lowers = [lower_ref[base + n] for n in range(group)]
        state = [[rhs_ref[base + n, 8 * b : 8 * b + 8] for b in range(SPAN // 8)] for n in range(group)]
        for s in range(SPAN - 1):
            for n in range(group):
                row = state[n][s // 8][s % 8 : s % 8 + 1]
                for b in range(s // 8 if s % 8 < 7 else s // 8 + 1, SPAN // 8):
                    state[n][b] = state[n][b] + lowers[n][8 * b : 8 * b + 8, s : s + 1] * row
        solved += [jnp.concatenate(one, axis=0) for one in state]
    prefix = jnp.where(diagonal, 1.0, 0.0).astype(F32)
    for c in range(count):
        got, moved = [], []
        for h in range(2):
            side_values = jnp.where(keep[h], 0.0, turned_ref[c])
            both = jnp.concatenate([solved[2 * c + h], side_values], axis=0)
            got.append(exact(reading_ref[2 * c + h], both))
            moved.append(exact(both, ends_ref[c], TN))
        lanes = lane_ids((128, 128)) < HD
        step = jnp.where(lanes, moved[0], moved[1]) + jnp.where(diagonal, last_ref[c, :1], 0.0)
        read_state = jnp.where(first, got[0], got[1]) + reads_ref[c]
        local = jnp.where(first, got[1], got[0])
        at = slice(c * SPAN, (c + 1) * SPAN)
        read_out[at, :] = exact(read_state, jnp.where(same, prefix, 0.0), NT)
        local_out[at, :] = local + exact(read_state, jnp.where(same, 0.0, prefix), NT)
        prefix = compose(prefix, step, same)
    message_out[:rows, :] = query_ref[...]
    message_out[rows:, :] = prefix.astype(BF16)


def along_x_kernel(place_ref, m0, m1, m2, m3, before_out, total_out, parts):
    rows = m0.shape[0] - 128
    same = same_head()
    identity = jnp.where(diagonal_mask(), 1.0, 0.0).astype(F32)
    mine = place_ref[1]
    for n, ref in enumerate((m0, m1, m2, m3)):
        parts[place_ref[10 + n]] = ref[rows:, :].astype(F32)
    total = compose(
        compose(parts[0], parts[1], same), compose(parts[2], parts[3], same), same
    ).astype(BF16)
    for n in range(8):
        total_out[n] = total
    kept = [jnp.where(j < mine, parts[j], identity) for j in range(3)]
    before_out[...] = compose(compose(kept[0], kept[1], same), kept[2], same)


def along_z_kernel(place_ref, parts_ref, before_ref, state_out):
    same = same_head()
    identity = jnp.where(diagonal_mask(), 1.0, 0.0).astype(F32)
    mine = place_ref[0]
    level = [jnp.where(j < mine, parts_ref[j].astype(F32), identity) for j in range(7)]
    level.append(before_ref[...])
    while len(level) > 1:
        level = [compose(level[i], level[i + 1], same) for i in range(0, len(level), 2)]
    state_out[...] = jnp.where(same, 0.0, level[0])


TALL = 144


def attention_kernel(blocks, is_first, is_last, *refs):
    place_ref, refs = refs[0], refs[1:]
    messages, refs = refs[:4], refs[4:]
    kvs, refs = refs[: len(blocks)], refs[len(blocks) :]
    if not is_first:
        (max_in, sum_in), refs = refs[:2], refs[2:]
    count = 4 if is_last else 2
    outs, refs = refs[:count], refs[count:]
    row_max, weighted, queries, keys, turned, scores, weights, rescales, units = refs
    rows = messages[0].shape[0] - 128
    my_z, my_x = place_ref[0], place_ref[1]
    first = lane_ids((rows, 128)) < HD
    for n, ref in enumerate(messages):
        scaled = (ref[:rows, :].astype(F32) * (HD**-0.5)).astype(BF16)
        queries[2 * n] = jnp.where(first, scaled, 0).astype(BF16)
        queries[2 * n + 1] = jnp.where(first, 0, scaled).astype(BF16)
    ones = jnp.where(row_ids((TALL - 128, rows)) == 0, 1.0, 0.0).astype(BF16)
    for n, ref in enumerate(kvs):
        keys[n] = ref[:, :128]
        turned[n, :128, :] = jnp.transpose(ref[:, 128:])
        turned[n, 128:, :] = ones
    if is_first:
        row_max[...] = jnp.full_like(row_max, NEGATIVE)
        weighted[...] = jnp.zeros_like(weighted)
    else:
        row_max[:8] = max_in[...]
        weighted[:8] = sum_in[...]

    def score(q, n, out):
        for m in range(2):
            out[m] = dot(keys[n], queries[2 * q + m], NT)

    def soften(slot, source, target, factors, diagonal=False):
        for m in range(2):
            i = 2 * slot + m
            got = source[m]
            if diagonal:
                allowed = row_ids((rows, rows)) <= lane_ids((rows, rows))
                got = jnp.where(allowed, got, NEGATIVE)
            old = row_max[i, :1, :]
            new = jnp.maximum(old, jnp.max(got, axis=0, keepdims=True))
            target[m] = jnp.exp(got - new).astype(BF16)
            factors[m] = jnp.broadcast_to(jnp.exp(old - new), (8, rows))
            row_max[i] = jnp.broadcast_to(new, (8, rows))

    def gather(slot, n, source, factors):
        for m in range(2):
            i = 2 * slot + m
            weighted[i] = weighted[i] * factors[m, :1, :] + dot(turned[n], source[m])

    def put(at, q, n, slot):
        units[0, at] = q
        units[1, at] = n
        units[2, at] = slot

    put(0, 0, 0, 4)
    total = jnp.int32(1)
    for n, number in enumerate(blocks):
        for q in range(4):
            put(total, q, n, q)
            wanted = place_ref[10 + q] > my_x if number == 0 else place_ref[2 + number] < my_z
            total = total + wanted.astype(jnp.int32)
    for extra in range(4):
        put(total + extra, 0, 0, 4)

    if is_first:
        score(0, 0, scores[0])
        soften(0, scores[0], weights[0], rescales[0], True)
        gather(0, 0, weights[0], rescales[0])

    @pl.when(total > 1)
    def _():
        score(units[0, 1], units[1, 1], scores[1])

        def step(at, now, other):
            score(units[0, at + 1], units[1, at + 1], scores[other])
            soften(units[2, at], scores[now], weights[now], rescales[now])
            gather(units[2, at - 1], units[1, at - 1], weights[other], rescales[other])

        def two(t, carry):
            step(2 * t + 1, 1, 0)
            step(2 * t + 2, 0, 1)
            return carry

        lax.fori_loop(0, (total + 1) // 2, two, 0)

    if is_last:
        for q, out in enumerate(outs):
            for m in range(2):
                i = 2 * q + m
                row_sum = weighted[i, 128:129, :]
                some = row_sum > 0.0
                safe = jnp.where(some, row_sum, 1.0)
                out[m, :128, :] = (weighted[i, :128, :] * (1.0 / safe)).astype(BF16)
                logs = jnp.where(some, row_max[i, :1, :] + jnp.log(safe), NEGATIVE)
                high = logs.astype(BF16).astype(F32)
                middle = (logs - high).astype(BF16).astype(F32)
                low = logs - high - middle
                tail = [high, middle, low, jnp.zeros((TALL - 131, rows), F32)]
                out[m, 128:, :] = jnp.concatenate(tail, axis=0).astype(BF16)
    else:
        outs[0][...] = row_max[:8]
        outs[1][...] = weighted[:8]


def finish_kernel(
    place_ref, lambda_ref, p0, p1, p2, p3, read_ref, local_ref, state_ref, wr_ref, wa_ref,
    mine_out, other_out, logs_out,
):
    rows = read_ref.shape[0]
    parts = (p0, p1, p2, p3)
    maps = []
    for m in range(2):
        logs = []
        for p in parts:
            tail = p[m, 128:, :].astype(F32)
            logs.append(tail[:1] + tail[1:2] + tail[2:3])
        top = functools.reduce(jnp.maximum, logs)
        shares = [jnp.exp(a - top) for a in logs]
        total = functools.reduce(jnp.add, shares)
        logs_out[m : m + 1, :] = top + jnp.log(total)
        got = None
        for p, share in zip(parts, shares):
            term = p[m, :128, :].astype(F32) * (share / total)
            got = term if got is None else got + term
        maps.append(got)
    head = maps[0] - lambda_ref[0] * maps[1]
    head = head * lax.rsqrt(jnp.mean(head * head, axis=0, keepdims=True) + HEAD_EPS)
    att_mix = jnp.transpose(head.astype(BF16))
    recurrent = local_ref[...] + exact(read_ref[...], state_ref[...], NT)
    recurrent = pltpu.roll(recurrent, HD, 1)
    first = lane_ids((rows, 128)) < HD

    def per_head(values):
        low = jnp.sum(jnp.where(first, values, 0.0), axis=-1, keepdims=True)
        high = jnp.sum(jnp.where(first, 0.0, values), axis=-1, keepdims=True)
        return jnp.where(first, low, high) / HD

    centered = recurrent - per_head(recurrent)
    rec_mix = (centered * lax.rsqrt(per_head(centered * centered) + GROUP_EPS)).astype(BF16)
    mix = jnp.concatenate([rec_mix, att_mix], axis=1)
    core = place_ref[0]
    for n in range(8):
        at = slice(256 * n, 256 * n + 256)
        weight = jnp.concatenate([wr_ref[:, at], wa_ref[:, at]], axis=0)
        got = dot(mix, weight).astype(BF16)
        for y in range(4):
            even = got[96 * y : 96 * y + 48]
            odd = got[96 * y + 48 : 96 * y + 96]
            mine_out[y, :, at] = jnp.where(core == 0, even, odd)
            other_out[y, :, at] = jnp.where(core == 0, odd, even)


def rms_rows(values, gain):
    return values * lax.rsqrt(jnp.mean(values * values, axis=-1, keepdims=True) + NORM_EPS) * gain


def per_device(
    hidden_in, in_gain, receptance_weight, key_weight, value_weight, decay_down, decay_up,
    decay_base, decay_shift, learn_rate, query_pair, key_pair, value_pair, mix_lambda,
    out_recurrent, out_attention, out_gain,
):
    permute = lax.ppermute
    together = lax.optimization_barrier
    z, x, y, core = (lax.axis_index(a) for a in ("z", "x", "y", "c"))
    rows = hidden_in.shape[0]
    half = rows // 2
    count = rows // SPAN
    shaped = jax.ShapeDtypeStruct

    up = permute(hidden_in, "y", ring(4, 1))
    down = permute(hidden_in, "y", ring(4, -1))
    far_a = permute(up[:half], "y", ring(4, 1))
    far_b = permute(down[half:], "y", ring(4, -1))
    mine = [hidden_in, up, down, far_a, far_b]
    theirs = [permute(a, "c", ring(2, 1)) for a in mine]
    ys = jnp.stack([y, (y + 3) % 4, (y + 1) % 4, (y + 2) % 4])
    piece_at = jnp.concatenate([ys * 2 + core, ys * 2 + 1 - core]).astype(jnp.int32)
    places = jnp.stack(
        [z, x, z]
        + [a for s in (1, 2, 3) for a in ((z + 8 - s) % 8, (z + s) % 8)]
        + [(z + 4) % 8, x, (x + 3) % 4, (x + 1) % 4, (x + 2) % 4]
    ).astype(jnp.int32)

    normed, q, kv = call(
        project_kernel,
        (shaped((rows, 2048), BF16), shaped((rows, 128), BF16), shaped((rows, 256), BF16)),
        (piece_at,),
        (
            *mine, *theirs, in_gain.reshape(8, 256), query_pair.reshape(2048, 128),
            key_pair.reshape(2048, 128), value_pair.reshape(2048, 128),
        ),
        flops=2 * rows * 2048 * 896,
        name="project",
    )

    right = permute(kv, "z", ring(8, 1))
    left = permute(kv, "z", ring(8, -1))
    tile = (2 * count, SPAN, 128)
    chunked = call(
        chunk_kernel,
        (
            shaped(tile, F32), shaped(tile, F32), shaped(tile, F32), shaped((count, SPAN, 128), F32),
            shaped((count, SPAN, 128), F32), shaped((count, 128, 128), F32), shaped((count, 8, 128), F32),
        ),
        (),
        (
            normed, receptance_weight, key_weight, value_weight, decay_down, decay_up,
            decay_base.reshape(1, 128), decay_shift, learn_rate.reshape(1, 128),
        ),
        flops=6 * 10**9,
        name="chunks",
    )
    right1, left1, chunked, q = together((right, left, chunked, q))
    right = permute(right1, "z", ring(8, 1))
    left = permute(left1, "z", ring(8, -1))
    read, local, message = call(
        recurrent_kernel,
        (shaped((rows, 128), F32), shaped((rows, 128), F32), shaped((rows + 128, 128), BF16)),
        (),
        (*chunked, q),
        flops=6 * 10**9,
        name="recurrent",
    )
    right2, left2, message = together((right, left, message))
    messages = [
        message,
        permute(message, "x", ring(4, 1)),
        permute(message, "x", ring(4, -1)),
        permute(message, "x", ring(4, 2)),
    ]
    right = permute(right2, "z", ring(8, 1))
    left = permute(left2, "z", ring(8, -1))
    before, line = call(
        along_x_kernel,
        (shaped((128, 128), F32), shaped((8, 128, 128), BF16)),
        (places,), messages, scratch=(pltpu.VMEM((4, 128, 128), F32),), flops=10**8, name="along_x",
    )
    right3, left3, line, messages = together((right, left, line, messages))
    line_parts = lax.all_to_all(line, "z", 0, 0, tiled=True)
    right4 = permute(right3, "z", ring(8, 1))

    carry = (shaped((8, 8, rows), F32), shaped((8, TALL, rows), F32))
    payload = shaped((2, TALL, rows), BF16)

    def attend(blocks, arrays, carried, last=False):
        pair = lambda shape, kind: [pltpu.VMEM(shape, kind)] * 2
        return call(
            functools.partial(attention_kernel, blocks, not carried, last),
            (payload,) * 4 if last else carry,
            (places,),
            (*messages, *arrays, *carried),
            scratch=[
                pltpu.VMEM((10, 8, rows), F32), pltpu.VMEM((10, TALL, rows), F32),
                pltpu.VMEM((8, rows, 128), BF16), pltpu.VMEM((len(blocks), rows, 128), BF16),
                pltpu.VMEM((len(blocks), TALL, rows), BF16), pair((2, rows, rows), F32),
                pair((2, rows, rows), BF16), pair((2, 8, rows), F32), pltpu.SMEM((3, 32), jnp.int32),
            ],
            flops=2 * len(blocks) * 10**9,
            name=f"attention{len(blocks)}",
        )

    carried = attend((0, 1, 2, 3, 4), (kv, right1, left1, right2, left2), ())
    outs = attend((5, 6, 7), (right3, left3, right4), tuple(carried), last=True)
    back = [
        outs[0],
        permute(outs[1], "x", ring(4, -1)),
        permute(outs[2], "x", ring(4, 1)),
        permute(outs[3], "x", ring(4, 2)),
    ]
    state = call(
        along_z_kernel, shaped((128, 128), F32), (places,), (line_parts, before),
        flops=10**8, name="along_z",
    )
    ours, others, log_sums = call(
        finish_kernel,
        (shaped((4, rows // 8, 2048), BF16), shaped((4, rows // 8, 2048), BF16), shaped((2, rows), F32)),
        (core.reshape(1), mix_lambda),
        (*back, read, local, state, out_recurrent, out_attention),
        flops=10**9,
        name="finish",
    )
    theirs = permute(others, "c", ring(2, 1))
    summed = (ours.astype(F32) + theirs.astype(F32)).astype(BF16)
    parts = lax.all_to_all(summed, "y", 0, 0, tiled=True)
    projected = jnp.sum(parts.astype(F32), axis=0)
    layer_out = rms_rows(projected, out_gain).astype(BF16)
    return (layer_out, log_sums[None])


def solution(mesh):
    split = Mesh(mesh.devices.reshape(8, 4, 4, 2), ("z", "x", "y", "c"))
    sp, tp = ("z", "x"), ("y", "c")
    placed = (
        P(sp, tp), P(), P(None, tp), P(None, tp), P(None, tp), P(), P(None, tp), P(tp), P(sp, tp),
        P(tp), P(None, tp, None), P(None, tp, None), P(None, tp, None), P(tp), P(tp, None),
        P(tp, None), P(),
    )
    return jax.shard_map(
        per_device,
        mesh=split,
        in_specs=placed,
        out_specs=(P(("z", "x", "y", "c"), None), P(tp, None, sp)),
        check_vma=False,
    )
```

```python
import functools
import math

import jax
import jax.numpy as jnp
from jax import lax
from jax.experimental import pallas as pl
from jax.experimental.pallas import tpu as pltpu
from jax.sharding import Mesh
from jax.sharding import PartitionSpec as P

HD = 64
F32 = jnp.float32
BF16 = jnp.bfloat16
DECAY_SCALE = math.exp(-0.5)
NORM_EPS = 1e-06
GROUP_EPS = 0.00064
HEAD_EPS = 1e-05
KEY_EPS = 1e-06
NEGATIVE = -1e30
SPAN = 64
GROUP = 12
MIB = 1024 * 1024
GRANT = 28
NT = (((1,), (1,)), ((), ()))
TN = (((0,), (0,)), ((), ()))
NN = (((1,), (0,)), ((), ()))


def call(kernel, outs, scalars, arrays, scratch=(), flops=0, grant=GRANT, name=None):
    return pl.pallas_call(
        kernel,
        out_shape=outs,
        in_specs=[pl.BlockSpec(memory_space=pltpu.SMEM)] * len(scalars)
        + [pl.BlockSpec(memory_space=pltpu.VMEM)] * len(arrays),
        out_specs=jax.tree.map(lambda _: pl.BlockSpec(memory_space=pltpu.VMEM), outs),
        scratch_shapes=list(scratch),
        compiler_params=pltpu.CompilerParams(vmem_limit_bytes=grant * MIB),
        cost_estimate=pl.CostEstimate(flops=flops, bytes_accessed=flops // 1000, transcendentals=0),
        name=name,
    )(*scalars, *arrays)


def dot(left, right, dims=NN):
    return lax.dot_general(left, right, dims, preferred_element_type=F32)


def halves(value):
    if value.dtype == BF16:
        return (value,)
    high = value.astype(BF16)
    return (high, (value - high.astype(F32)).astype(BF16))


def exact(left, right, dims=NN):
    left, right = halves(left), halves(right)
    total = dot(left[0], right[0], dims)
    for more in left[1:]:
        total = total + dot(more, right[0], dims)
    for more in right[1:]:
        total = total + dot(left[0], more, dims)
    return total


def ring(size, shift):
    return [(i, (i + shift) % size) for i in range(size)]


def lane_ids(shape):
    return lax.broadcasted_iota(jnp.int32, shape, len(shape) - 1)


def row_ids(shape):
    return lax.broadcasted_iota(jnp.int32, shape, len(shape) - 2)


def project_kernel(
    piece_ref,
    own, h1, h2, h3, h4, g0, g1, g2, g3, g4, gain_ref, weights,
    normed, q_out, kv_out,
):
    half = own.shape[0] // 2
    pieces = [
        h1[...], h2[...], jnp.concatenate([h3[...], h4[...]], axis=0),
        g0[...], g1[...], g2[...], jnp.concatenate([g3[...], g4[...]], axis=0),
        jnp.concatenate([own[half:], own[:half]], axis=0),
    ]
    squares = None
    for piece in pieces:
        wide = piece.astype(F32)
        part = wide * wide
        part = part[:, :128] + part[:, 128:]
        squares = part if squares is None else squares + part
    scale = lax.rsqrt(jnp.sum(squares, axis=-1, keepdims=True) / 2048.0 + NORM_EPS)
    for number, piece in enumerate(pieces):
        place = piece_ref[number]
        gain = gain_ref[pl.ds(place, 1), :]
        value = (piece.astype(F32) * scale * gain).astype(BF16)
        normed[:, pl.ds(pl.multiple_of(place * 256, 256), 256)] = value
    kv_out[...] = dot(normed[...], weights[:, :256]).astype(BF16)
    q_out[...] = dot(normed[...], weights[:, 256:]).astype(BF16)


def same_head():
    return (row_ids((128, 128)) < HD) == (lane_ids((128, 128)) < HD)


def diagonal_mask():
    return row_ids((128, 128)) == lane_ids((128, 128))


def compose(earlier, later, same):
    zero = jnp.zeros_like(later)
    return exact(earlier, jnp.where(same, later, zero)) + jnp.where(same, zero, later).astype(F32)


def chunk_kernel(
    normed, wr, wk, wv, wd, up_ref, base_ref, shift_ref, rate_ref,
    lower_out, reading_out, rhs_out, turned_out, reads_out, ends_out, last_out,
):
    both = dot(normed[...], jnp.concatenate([wr[...], wk[...]], axis=1))
    all_reads = both[:, :128].astype(BF16)
    all_keys = both[:, 128:].astype(BF16)
    both = dot(normed[...], jnp.concatenate([wv[...], wd[...]], axis=1))
    all_values = both[:, :128].astype(BF16)
    low = jnp.tanh(both[:, 128:]).astype(BF16)
    pre = dot(low, up_ref[...]) + base_ref[...]
    all_decay = -DECAY_SCALE * jax.nn.sigmoid(pre) + shift_ref[...]
    rows = normed.shape[0]
    count = rows // SPAN
    ones_block = jnp.where(same_head(), 1.0, 0.0).astype(BF16)
    first = lane_ids((SPAN, 128)) < HD
    t_ids = row_ids((SPAN, 128))
    s_ids = lane_ids((SPAN, 128)) % HD
    strict = s_ids < t_ids
    causal = s_ids <= t_ids
    tri = jnp.where(row_ids((SPAN, SPAN)) >= lane_ids((SPAN, SPAN)), 1.0, 0.0).astype(BF16)
    keep = (first, jnp.logical_not(first))
    zero = jnp.zeros((SPAN, 128), F32)
    for c in range(count):
        at = slice(c * SPAN, (c + 1) * SPAN)
        decay = all_decay[at, :]
        running = exact(tri, decay)
        before = running - decay
        middle = running[SPAN // 2 - 1 : SPAN // 2, :]
        ending = running[SPAN - 1 : SPAN, :]
        keys = all_keys[at, :].astype(F32)
        reads = all_reads[at, :].astype(F32)
        values = all_values[at, :].astype(F32)
        unit_keys = keys * lax.rsqrt(exact(keys * keys, ones_block) + KEY_EPS)
        erasing = unit_keys * rate_ref[...]
        grow = jnp.exp(middle - running)
        against = -unit_keys * jnp.exp(before - middle)
        read_scaled = reads * jnp.exp(running - middle)
        right = jnp.concatenate([erasing * grow, keys * grow], axis=0)
        left = jnp.concatenate(
            [jnp.where(k, side, 0.0) for k in keep for side in (against, read_scaled)], axis=0
        )
        scores = exact(left, right, NT)
        turned = pltpu.roll(values, HD, 1)
        to_end = jnp.exp(ending - running)
        ends_out[c] = jnp.concatenate([erasing * to_end, keys * to_end], axis=0)
        start = -unit_keys * jnp.exp(before)
        reads_out[c] = reads * jnp.exp(running)
        last_out[c] = jnp.broadcast_to(jnp.exp(ending), (8, 128))
        turned_out[c] = turned
        for h in range(2):
            lower = jnp.where(strict, scores[128 * h : 128 * h + SPAN], 0.0)
            lower_out[2 * c + h] = lower
            reading_out[2 * c + h] = jnp.where(causal, scores[128 * h + SPAN : 128 * h + 128], 0.0)
            side_values = jnp.where(keep[h], 0.0, turned)
            rhs_out[2 * c + h] = jnp.where(keep[h], start, 0.0) + exact(
                lower, jnp.concatenate([zero, side_values], axis=0).astype(BF16)
            )


def recurrent_kernel(
    lower_ref, reading_ref, rhs_ref, turned_ref, reads_ref, ends_ref, last_ref, query_ref,
    read_out, local_out, message_out,
):
    count = turned_ref.shape[0]
    rows = count * SPAN
    same = same_head()
    diagonal = diagonal_mask()
    first = lane_ids((SPAN, 128)) < HD
    keep = (first, jnp.logical_not(first))
    solved = []
    group = GROUP
    for base in range(0, 2 * count, group):
        lowers = [lower_ref[base + n] for n in range(group)]
        state = [[rhs_ref[base + n, 8 * b : 8 * b + 8] for b in range(SPAN // 8)] for n in range(group)]
        for s in range(SPAN - 1):
            for n in range(group):
                row = state[n][s // 8][s % 8 : s % 8 + 1]
                for b in range(s // 8 if s % 8 < 7 else s // 8 + 1, SPAN // 8):
                    state[n][b] = state[n][b] + lowers[n][8 * b : 8 * b + 8, s : s + 1] * row
        solved += [jnp.concatenate(one, axis=0) for one in state]
    prefix = jnp.where(diagonal, 1.0, 0.0).astype(F32)
    for c in range(count):
        got, moved = [], []
        for h in range(2):
            side_values = jnp.where(keep[h], 0.0, turned_ref[c])
            both = jnp.concatenate([solved[2 * c + h], side_values], axis=0)
            got.append(exact(reading_ref[2 * c + h], both))
            moved.append(exact(both, ends_ref[c], TN))
        lanes = lane_ids((128, 128)) < HD
        step = jnp.where(lanes, moved[0], moved[1]) + jnp.where(diagonal, last_ref[c, :1], 0.0)
        read_state = jnp.where(first, got[0], got[1]) + reads_ref[c]
        local = jnp.where(first, got[1], got[0])
        at = slice(c * SPAN, (c + 1) * SPAN)
        read_out[at, :] = exact(read_state, jnp.where(same, prefix, 0.0), NT)
        local_out[at, :] = local + exact(read_state, jnp.where(same, 0.0, prefix), NT)
        prefix = compose(prefix, step, same)
    message_out[:rows, :] = query_ref[...]
    message_out[rows:, :] = prefix.astype(BF16)


def along_x_kernel(place_ref, m0, m1, m2, m3, before_out, total_out, parts):
    rows = m0.shape[0] - 128
    same = same_head()
    identity = jnp.where(diagonal_mask(), 1.0, 0.0).astype(BF16)
    mine = place_ref[1]
    for n, ref in enumerate((m0, m1, m2, m3)):
        parts[place_ref[10 + n]] = ref[rows:, :]
    total = parts[0]
    for j in range(1, 4):
        total = compose(total, parts[j], same)
    for n in range(8):
        total_out[n] = total.astype(BF16)
    before = jnp.where(mine > 0, parts[0], identity)
    for j in range(1, 3):
        before = compose(before, jnp.where(j < mine, parts[j], identity), same)
    before_out[...] = before


def along_z_kernel(place_ref, parts_ref, before_ref, state_out):
    same = same_head()
    identity = jnp.where(diagonal_mask(), 1.0, 0.0).astype(BF16)
    mine = place_ref[0]
    level = [jnp.where(j < mine, parts_ref[j], identity) for j in range(7)]
    level.append(before_ref[...])
    while len(level) > 1:
        level = [compose(level[i], level[i + 1], same) for i in range(0, len(level), 2)]
    state_out[...] = jnp.where(same, 0.0, level[0])


TALL = 144


def attention_kernel(
    place_ref, m0, m1, m2, m3, *refs
):
    kvs, outs = refs[:8], refs[8:12]
    row_max, weighted, queries, keys, turned, scores, weights, rescales, units = refs[12:]
    rows = m0.shape[0] - 128
    wide = 2 * rows
    my_z, my_x = place_ref[0], place_ref[1]
    first = lane_ids((rows, 128)) < HD
    for n, ref in enumerate((m0, m1, m2, m3)):
        scaled = (ref[:rows, :].astype(F32) * (HD**-0.5)).astype(BF16)
        at = slice((n % 2) * rows, (n % 2 + 1) * rows)
        queries[2 * (n // 2), at, :] = jnp.where(first, scaled, 0).astype(BF16)
        queries[2 * (n // 2) + 1, at, :] = jnp.where(first, 0, scaled).astype(BF16)
    ones = jnp.where(row_ids((TALL - 128, rows)) == 0, 1.0, 0.0).astype(BF16)
    for n, ref in enumerate(kvs):
        keys[n] = ref[:, :128]
        turned[n, :128, :] = jnp.transpose(ref[:, 128:])
        turned[n, 128:, :] = ones
    row_max[...] = jnp.full_like(row_max, NEGATIVE)
    weighted[...] = jnp.zeros_like(weighted)

    def score(pair, n, out):
        for m in range(2):
            out[m] = dot(keys[n], queries[2 * pair + m], NT)

    def soften(slot, source, target, factors, limit=None):
        for m in range(2):
            i = 2 * slot + m
            got = source[m]
            if limit is not None:
                got = jnp.where(row_ids((rows, wide)) <= limit, got, NEGATIVE)
            old = row_max[i, :1, :]
            new = jnp.maximum(old, jnp.max(got, axis=0, keepdims=True))
            target[m] = jnp.exp(got - new).astype(BF16)
            factors[m] = jnp.broadcast_to(jnp.exp(old - new), (8, wide))
            row_max[i] = jnp.broadcast_to(new, (8, wide))

    def gather(slot, n, source, factors):
        for m in range(2):
            i = 2 * slot + m
            weighted[i] = weighted[i] * factors[m, :1, :] + dot(turned[n], source[m])

    def put(at, pair, n, slot):
        units[0, at] = pair
        units[1, at] = n
        units[2, at] = slot

    put(0, 1, 0, 1)
    total = jnp.int32(1)
    for n in range(1, 8):
        wanted = place_ref[2 + n] < my_z
        for pair in range(2):
            put(total, pair, n, pair)
            total = total + wanted.astype(jnp.int32)
    for extra in range(4):
        put(total + extra, 0, 0, 2)

    column = lane_ids((1, wide))
    within = jnp.where(column < rows, column, column - rows)

    def limit(pair):
        x_of = jnp.where(column < rows, place_ref[10 + 2 * pair], place_ref[11 + 2 * pair])
        return jnp.where(x_of > my_x, rows, jnp.where(x_of == my_x, within, -1))

    score(0, 0, scores[0])
    score(1, 0, scores[1])
    soften(0, scores[0], weights[0], rescales[0], limit(0))
    score(units[0, 1], units[1, 1], scores[0])
    soften(1, scores[1], weights[1], rescales[1], limit(1))
    gather(0, 0, weights[0], rescales[0])

    def step(at, now, other):
        score(units[0, at + 1], units[1, at + 1], scores[other])
        soften(units[2, at], scores[now], weights[now], rescales[now])
        gather(units[2, at - 1], units[1, at - 1], weights[other], rescales[other])

    def two(t, carry):
        step(2 * t + 1, 0, 1)
        step(2 * t + 2, 1, 0)
        return carry

    lax.fori_loop(0, (total + 1) // 2, two, 0)

    for n, out in enumerate(outs):
        at = slice((n % 2) * rows, (n % 2 + 1) * rows)
        for m in range(2):
            i = 2 * (n // 2) + m
            top = row_max[i, :1, at]
            some = top > 0.5 * NEGATIVE
            row_sum = jnp.where(some, weighted[i, 128:129, at], 1.0)
            share = jnp.where(some, 1.0 / row_sum, 0.0)
            out[m, :128, :] = (weighted[i, :128, at] * share).astype(BF16)
            logs = jnp.where(some, top + jnp.log(row_sum), NEGATIVE)
            high = logs.astype(BF16).astype(F32)
            middle = (logs - high).astype(BF16).astype(F32)
            low = logs - high - middle
            tail = [high, middle, low, jnp.zeros((TALL - 131, rows), F32)]
            out[m, 128:, :] = jnp.concatenate(tail, axis=0).astype(BF16)


def finish_kernel(
    place_ref, lambda_ref, p0, p1, p2, p3, read_ref, local_ref, state_ref, wr_ref, wa_ref,
    mine_out, other_out, logs_out,
):
    rows = read_ref.shape[0]
    parts = (p0, p1, p2, p3)
    maps = []
    for m in range(2):
        logs = []
        for p in parts:
            tail = p[m, 128:, :].astype(F32)
            logs.append(tail[:1] + tail[1:2] + tail[2:3])
        top = functools.reduce(jnp.maximum, logs)
        shares = [jnp.exp(a - top) for a in logs]
        total = functools.reduce(jnp.add, shares)
        logs_out[m : m + 1, :] = top + jnp.log(total)
        got = None
        for p, share in zip(parts, shares):
            term = p[m, :128, :].astype(F32) * (share / total)
            got = term if got is None else got + term
        maps.append(got)
    head = maps[0] - lambda_ref[0] * maps[1]
    head = head * lax.rsqrt(jnp.mean(head * head, axis=0, keepdims=True) + HEAD_EPS)
    att_mix = jnp.transpose(head.astype(BF16))
    recurrent = local_ref[...] + exact(read_ref[...], state_ref[...], NT)
    recurrent = pltpu.roll(recurrent, HD, 1)
    first = lane_ids((rows, 128)) < HD

    def per_head(values):
        low = jnp.sum(jnp.where(first, values, 0.0), axis=-1, keepdims=True)
        high = jnp.sum(jnp.where(first, 0.0, values), axis=-1, keepdims=True)
        return jnp.where(first, low, high) / HD

    centered = recurrent - per_head(recurrent)
    rec_mix = (centered * lax.rsqrt(per_head(centered * centered) + GROUP_EPS)).astype(BF16)
    mix = jnp.concatenate([rec_mix, att_mix], axis=1)
    core = place_ref[0]
    for n in range(8):
        at = slice(256 * n, 256 * n + 256)
        weight = jnp.concatenate([wr_ref[:, at], wa_ref[:, at]], axis=0)
        got = dot(mix, weight).astype(BF16)
        for y in range(4):
            even = got[96 * y : 96 * y + 48]
            odd = got[96 * y + 48 : 96 * y + 96]
            mine_out[y, :, at] = jnp.where(core == 0, even, odd)
            other_out[y, :, at] = jnp.where(core == 0, odd, even)


def rms_rows(values, gain):
    return values * lax.rsqrt(jnp.mean(values * values, axis=-1, keepdims=True) + NORM_EPS) * gain


def per_device(
    hidden_in, in_gain, receptance_weight, key_weight, value_weight, decay_down, decay_up,
    decay_base, decay_shift, learn_rate, query_pair, key_pair, value_pair, mix_lambda,
    out_recurrent, out_attention, out_gain,
):
    permute = lax.ppermute
    together = lax.optimization_barrier
    z, x, y, core = (lax.axis_index(a) for a in ("z", "x", "y", "c"))
    rows = hidden_in.shape[0]
    half = rows // 2
    count = rows // SPAN
    shaped = jax.ShapeDtypeStruct

    up = permute(hidden_in, "y", ring(4, 1))
    down = permute(hidden_in, "y", ring(4, -1))
    far_a = permute(up[:half], "y", ring(4, 1))
    far_b = permute(down[half:], "y", ring(4, -1))
    mine = [up, down, far_a, far_b]
    theirs = [permute(a, "c", ring(2, 1)) for a in (hidden_in, *mine)]
    ys = [(y + 3) % 4, (y + 1) % 4, (y + 2) % 4, y]
    piece_at = jnp.stack(
        [2 * a + core for a in ys[:3]] + [2 * a + 1 - core for a in (y, *ys[:3])] + [2 * y + core]
    ).astype(jnp.int32)
    places = jnp.stack(
        [z, x, z]
        + [a for s in (1, 2, 3) for a in ((z + 8 - s) % 8, (z + s) % 8)]
        + [(z + 4) % 8, x, (x + 3) % 4, (x + 1) % 4, (x + 2) % 4]
    ).astype(jnp.int32)

    turned_in = jnp.concatenate([hidden_in[half:], hidden_in[:half]], axis=0)
    pair_weights = jnp.concatenate([key_pair, value_pair, query_pair], axis=2).reshape(2048, 384)
    normed, q, kv = call(
        project_kernel,
        (shaped((rows, 2048), BF16), shaped((rows, 128), BF16), shaped((rows, 256), BF16)),
        (piece_at,),
        (turned_in, *mine, *theirs, in_gain.reshape(8, 256), pair_weights),
        flops=2 * rows * 2048 * 896,
        name="project",
    )

    right = permute(kv, "z", ring(8, 1))
    left = permute(kv, "z", ring(8, -1))
    tile = (2 * count, SPAN, 128)
    chunked = call(
        chunk_kernel,
        (
            shaped(tile, F32), shaped(tile, F32), shaped(tile, F32), shaped((count, SPAN, 128), F32),
            shaped((count, SPAN, 128), F32), shaped((count, 128, 128), F32), shaped((count, 8, 128), F32),
        ),
        (),
        (
            normed, receptance_weight, key_weight, value_weight, decay_down, decay_up,
            decay_base.reshape(1, 128), decay_shift, learn_rate.reshape(1, 128),
        ),
        flops=6 * 10**9,
        name="chunks",
    )
    right1, left1, chunked, q = together((right, left, chunked, q))
    right = permute(right1, "z", ring(8, 1))
    left = permute(left1, "z", ring(8, -1))
    read, local, message = call(
        recurrent_kernel,
        (shaped((rows, 128), F32), shaped((rows, 128), F32), shaped((rows + 128, 128), BF16)),
        (),
        (*chunked, q),
        flops=6 * 10**9,
        name="recurrent",
    )
    right2, left2, message = together((right, left, message))
    right = permute(right2, "z", ring(8, 1))
    left = permute(left2, "z", ring(8, -1))
    messages = [
        message,
        permute(message, "x", ring(4, 1)),
        permute(message, "x", ring(4, -1)),
        permute(message, "x", ring(4, 2)),
    ]
    right3, left3, messages = together((right, left, messages))
    right4 = permute(right3, "z", ring(8, 1))
    before, line = call(
        along_x_kernel,
        (shaped((128, 128), F32), shaped((8, 128, 128), BF16)),
        (places,), messages, scratch=(pltpu.VMEM((4, 128, 128), BF16),), flops=10**8, name="along_x",
    )
    line_parts = lax.all_to_all(line, "z", 0, 0, tiled=True)

    payload = shaped((2, TALL, rows), BF16)
    wide = 2 * rows

    def pair(shape, kind):
        return [pltpu.VMEM(shape, kind)] * 2

    outs = call(
        attention_kernel,
        (payload,) * 4,
        (places,),
        (*messages, kv, right1, left1, right2, left2, right3, left3, right4),
        scratch=[
            pltpu.VMEM((6, 8, wide), F32), pltpu.VMEM((6, TALL, wide), F32),
            pltpu.VMEM((4, wide, 128), BF16), pltpu.VMEM((8, rows, 128), BF16),
            pltpu.VMEM((8, TALL, rows), BF16), pair((2, rows, wide), F32),
            pair((2, rows, wide), BF16), pair((2, 8, wide), F32), pltpu.SMEM((3, 32), jnp.int32),
        ],
        flops=16 * 10**9,
        name="attention",
    )
    back = [
        outs[0],
        permute(outs[1], "x", ring(4, -1)),
        permute(outs[2], "x", ring(4, 1)),
        permute(outs[3], "x", ring(4, 2)),
    ]
    state = call(
        along_z_kernel, shaped((128, 128), F32), (places,), (line_parts, before),
        flops=10**8, name="along_z",
    )
    ours, others, log_sums = call(
        finish_kernel,
        (shaped((4, rows // 8, 2048), BF16), shaped((4, rows // 8, 2048), BF16), shaped((2, rows), F32)),
        (core.reshape(1), mix_lambda),
        (*back, read, local, state, out_recurrent, out_attention),
        flops=10**9,
        name="finish",
    )
    theirs = permute(others, "c", ring(2, 1))
    summed = (ours.astype(F32) + theirs.astype(F32)).astype(BF16)
    parts = lax.all_to_all(summed, "y", 0, 0, tiled=True)
    projected = jnp.sum(parts.astype(F32), axis=0)
    layer_out = rms_rows(projected, out_gain).astype(BF16)
    return (layer_out, log_sums[None])


def solution(mesh):
    split = Mesh(mesh.devices.reshape(8, 4, 4, 2), ("z", "x", "y", "c"))
    sp, tp = ("z", "x"), ("y", "c")
    placed = (
        P(sp, tp), P(), P(None, tp), P(None, tp), P(None, tp), P(), P(None, tp), P(tp), P(sp, tp),
        P(tp), P(None, tp, None), P(None, tp, None), P(None, tp, None), P(tp), P(tp, None),
        P(tp, None), P(),
    )
    return jax.shard_map(
        per_device,
        mesh=split,
        in_specs=placed,
        out_specs=(P(("z", "x", "y", "c"), None), P(tp, None, sp)),
        check_vma=False,
    )
```

```python
import functools
import math

import jax
import jax.numpy as jnp
from jax import lax
from jax.experimental import pallas as pl
from jax.experimental.pallas import tpu as pltpu
from jax.sharding import Mesh
from jax.sharding import PartitionSpec as P

HD = 64
F32 = jnp.float32
BF16 = jnp.bfloat16
DECAY_SCALE = math.exp(-0.5)
NORM_EPS = 1e-06
GROUP_EPS = 0.00064
HEAD_EPS = 1e-05
KEY_EPS = 1e-06
NEGATIVE = -1e30
SPAN = 64
MIB = 1024 * 1024
GRANT = 28
NT = (((1,), (1,)), ((), ()))
TN = (((0,), (0,)), ((), ()))
NN = (((1,), (0,)), ((), ()))


def call(kernel, outs, scalars, arrays, scratch=(), flops=0, grant=GRANT, name=None):
    return pl.pallas_call(
        kernel,
        out_shape=outs,
        in_specs=[pl.BlockSpec(memory_space=pltpu.SMEM)] * len(scalars)
        + [pl.BlockSpec(memory_space=pltpu.VMEM)] * len(arrays),
        out_specs=jax.tree.map(lambda _: pl.BlockSpec(memory_space=pltpu.VMEM), outs),
        scratch_shapes=list(scratch),
        compiler_params=pltpu.CompilerParams(vmem_limit_bytes=grant * MIB),
        cost_estimate=pl.CostEstimate(flops=flops, bytes_accessed=flops // 1000, transcendentals=0),
        name=name,
    )(*scalars, *arrays)


def dot(left, right, dims=NN):
    return lax.dot_general(left, right, dims, preferred_element_type=F32)


def halves(value):
    if value.dtype == BF16:
        return (value,)
    high = value.astype(BF16)
    return (high, (value - high.astype(F32)).astype(BF16))


def exact(left, right, dims=NN):
    left, right = halves(left), halves(right)
    total = dot(left[0], right[0], dims)
    for more in left[1:]:
        total = total + dot(more, right[0], dims)
    for more in right[1:]:
        total = total + dot(left[0], more, dims)
    return total


def ring(size, shift):
    return [(i, (i + shift) % size) for i in range(size)]


def lane_ids(shape):
    return lax.broadcasted_iota(jnp.int32, shape, len(shape) - 1)


def row_ids(shape):
    return lax.broadcasted_iota(jnp.int32, shape, len(shape) - 2)


def project_kernel(
    own, h1, h2, h3, g0, g1, g2, g3, gain_ref, weights,
    normed, q_out, kv_out,
):
    half = own.shape[0] // 2
    pieces = [
        h1[...], h2[...], h3[...],
        g0[...], g1[...], g2[...], g3[...],
        jnp.concatenate([own[half:], own[:half]], axis=0),
    ]
    squares = None
    for piece in pieces:
        wide = piece.astype(F32)
        part = wide * wide
        part = part[:, :128] + part[:, 128:]
        squares = part if squares is None else squares + part
    scale = lax.rsqrt(jnp.sum(squares, axis=-1, keepdims=True) / 2048.0 + NORM_EPS)
    y, core = lax.axis_index("y"), lax.axis_index("c")
    ys = [(y + 3) & 3, (y + 1) & 3, (y + 2) & 3]
    places = [2 * a + core for a in ys] + [2 * a + 1 - core for a in (y, *ys)] + [2 * y + core]
    for place, piece in zip(places, pieces):
        gain = gain_ref[pl.ds(place, 1), :]
        value = (piece.astype(F32) * scale * gain).astype(BF16)
        normed[:, pl.ds(pl.multiple_of(place * 256, 256), 256)] = value
    kv_out[...] = dot(normed[...], weights[:, :256]).astype(BF16)
    q_out[...] = dot(normed[...], weights[:, 256:]).astype(BF16)


def line_places():
    x = lax.axis_index("x")
    return [x, (x + 3) & 3, (x + 1) & 3, (x + 2) & 3]


def ring_places():
    z = lax.axis_index("z")
    return [z] + [(z + 8 + s) & 7 for s in (-1, 1, -2, 2, -3, 3, 4)]


def same_head():
    return (row_ids((128, 128)) < HD) == (lane_ids((128, 128)) < HD)


def diagonal_mask():
    return row_ids((128, 128)) == lane_ids((128, 128))


def compose(earlier, later, same):
    zero = jnp.zeros_like(later)
    return exact(earlier, jnp.where(same, later, zero)) + jnp.where(same, zero, later).astype(F32)


def chunk_kernel(
    normed, wr, wk, wv, wd, up_ref, base_ref, shift_ref, rate_ref,
    lower_out, reading_out, rhs_out, turned_out, reads_out, ends_out, last_out,
):
    both = dot(normed[...], jnp.concatenate([wr[...], wk[...]], axis=1))
    all_reads = both[:, :128].astype(BF16)
    all_keys = both[:, 128:].astype(BF16)
    both = dot(normed[...], jnp.concatenate([wv[...], wd[...]], axis=1))
    all_values = both[:, :128].astype(BF16)
    low = jnp.tanh(both[:, 128:]).astype(BF16)
    pre = dot(low, up_ref[...]) + base_ref[...]
    all_decay = -DECAY_SCALE * jax.nn.sigmoid(pre) + shift_ref[...]
    rows = normed.shape[0]
    count = rows // SPAN
    ones_block = jnp.where(same_head(), 1.0, 0.0).astype(BF16)
    first = lane_ids((SPAN, 128)) < HD
    t_ids = row_ids((SPAN, 128))
    s_ids = lane_ids((SPAN, 128)) % HD
    strict = s_ids < t_ids
    causal = s_ids <= t_ids
    tri = jnp.where(row_ids((SPAN, SPAN)) >= lane_ids((SPAN, SPAN)), 1.0, 0.0).astype(BF16)
    keep = (first, jnp.logical_not(first))
    zero = jnp.zeros((SPAN, 128), F32)
    for c in range(count):
        at = slice(c * SPAN, (c + 1) * SPAN)
        decay = all_decay[at, :]
        running = exact(tri, decay)
        before = running - decay
        middle = running[SPAN // 2 - 1 : SPAN // 2, :]
        ending = running[SPAN - 1 : SPAN, :]
        keys = all_keys[at, :].astype(F32)
        reads = all_reads[at, :].astype(F32)
        values = all_values[at, :].astype(F32)
        unit_keys = keys * lax.rsqrt(exact(keys * keys, ones_block) + KEY_EPS)
        erasing = unit_keys * rate_ref[...]
        grow = jnp.exp(middle - running)
        against = -unit_keys * jnp.exp(before - middle)
        read_scaled = reads * jnp.exp(running - middle)
        right = jnp.concatenate([erasing * grow, keys * grow], axis=0)
        left = jnp.concatenate(
            [jnp.where(k, side, 0.0) for k in keep for side in (against, read_scaled)], axis=0
        )
        scores = exact(left, right, NT)
        turned = pltpu.roll(values, HD, 1)
        to_end = jnp.exp(ending - running)
        ends_out[c] = jnp.concatenate([erasing * to_end, keys * to_end], axis=0)
        start = -unit_keys * jnp.exp(before)
        reads_out[c] = reads * jnp.exp(running)
        last_out[c] = jnp.broadcast_to(jnp.exp(ending), (8, 128))
        turned_out[c] = turned
        for h in range(2):
            lower = jnp.where(strict, scores[128 * h : 128 * h + SPAN], 0.0)
            lower_out[2 * c + h] = lower
            reading_out[2 * c + h] = jnp.where(causal, scores[128 * h + SPAN : 128 * h + 128], 0.0)
            side_values = jnp.where(keep[h], 0.0, turned)
            rhs_out[2 * c + h] = jnp.where(keep[h], start, 0.0) + exact(
                lower, jnp.concatenate([zero, side_values], axis=0).astype(BF16)
            )


def recurrent_kernel(
    lower_ref, reading_ref, rhs_ref, turned_ref, reads_ref, ends_ref, last_ref, query_ref,
    read_out, local_out, message_out,
):
    count = turned_ref.shape[0]
    rows = count * SPAN
    same = same_head()
    diagonal = diagonal_mask()
    first = lane_ids((SPAN, 128)) < HD
    keep = (first, jnp.logical_not(first))
    units = range(2 * count)
    lowers = [lower_ref[n] for n in units]
    state = [[rhs_ref[n, 8 * b : 8 * b + 8] for b in range(SPAN // 8)] for n in units]
    half = SPAN // 2

    def substitute(start):
        for s in range(start, start + half - 1):
            for n in units:
                row = state[n][s // 8][s % 8 : s % 8 + 1]
                for b in range(s // 8 if s % 8 < 7 else s // 8 + 1, (start + half) // 8):
                    state[n][b] = state[n][b] + lowers[n][8 * b : 8 * b + 8, s : s + 1] * row

    substitute(0)
    rest = jnp.zeros((128 - half, 128), F32)
    for n in units:
        above = jnp.concatenate(state[n][: half // 8] + [rest], axis=0)
        more = exact(lowers[n][half:], above)
        for b in range(half // 8, SPAN // 8):
            state[n][b] = state[n][b] + more[8 * b - half : 8 * b - half + 8]
    substitute(half)
    solved = [jnp.concatenate(one, axis=0) for one in state]
    prefix = jnp.where(diagonal, 1.0, 0.0).astype(F32)
    for c in range(count):
        got, moved = [], []
        for h in range(2):
            side_values = jnp.where(keep[h], 0.0, turned_ref[c])
            both = jnp.concatenate([solved[2 * c + h], side_values], axis=0)
            got.append(exact(reading_ref[2 * c + h], both))
            moved.append(exact(both, ends_ref[c], TN))
        lanes = lane_ids((128, 128)) < HD
        step = jnp.where(lanes, moved[0], moved[1]) + jnp.where(diagonal, last_ref[c, :1], 0.0)
        read_state = jnp.where(first, got[0], got[1]) + reads_ref[c]
        local = jnp.where(first, got[1], got[0])
        at = slice(c * SPAN, (c + 1) * SPAN)
        read_out[at, :] = exact(read_state, jnp.where(same, prefix, 0.0), NT)
        local_out[at, :] = local + exact(read_state, jnp.where(same, 0.0, prefix), NT)
        prefix = compose(prefix, step, same)
    message_out[:rows, :] = query_ref[...]
    message_out[rows:, :] = prefix.astype(BF16)


def along_x_kernel(m0, m1, m2, m3, before_out, total_out, parts):
    rows = m0.shape[0] - 128
    same = same_head()
    identity = jnp.where(diagonal_mask(), 1.0, 0.0).astype(BF16)
    mine = lax.axis_index("x")
    for place, ref in zip(line_places(), (m0, m1, m2, m3)):
        parts[place] = ref[rows:, :]
    total = parts[0]
    for j in range(1, 4):
        total = compose(total, parts[j], same)
    total_out[...] = total.astype(BF16)
    before = jnp.where(mine > 0, parts[0], identity)
    for j in range(1, 3):
        before = compose(before, jnp.where(j < mine, parts[j], identity), same)
    before_out[...] = before


def window_kernel(line_ref, p1, p2, p3, window_out, near_out):
    same = same_head()
    identity = jnp.where(diagonal_mask(), 1.0, 0.0).astype(BF16)
    mine = lax.axis_index("z")
    near = jnp.where(mine >= 3, p3[...], identity)
    for far, part in ((2, p2), (1, p1)):
        near = compose(near, jnp.where(mine >= far, part[...], identity), same)
    near_out[...] = near
    window_out[...] = compose(near, line_ref[...], same).astype(BF16)


def state_before(window, near, before):
    same = same_head()
    identity = jnp.where(diagonal_mask(), 1.0, 0.0).astype(BF16)
    window = jnp.where(lax.axis_index("z") >= 4, window, identity)
    total = compose(compose(window, near, same), before, same)
    return jnp.where(same, 0.0, total)


TALL = 144


def attention_kernel(pair, *refs):
    lead, refs = refs[:2], refs[2:]
    taken = 8 if pair else 2
    kvs, refs = refs[:taken], refs[taken:]
    outs, refs = refs[:2], refs[2:]
    keys, turned = refs[:2] if pair else kvs
    row_max, weighted, queries, scores, units = refs[2:] if pair else refs
    rows = lead[0].shape[0] - 128
    wide = 2 * rows
    blocks_at, lines_at = ring_places(), line_places()
    my_z, my_x = blocks_at[0], lines_at[0]
    first = lane_ids((rows, 128)) < HD
    for n, ref in enumerate(lead):
        scaled = (ref[:rows, :].astype(F32) * (HD**-0.5)).astype(BF16)
        at = slice(n * rows, (n + 1) * rows)
        queries[0, at, :] = jnp.where(first, scaled, 0).astype(BF16)
        queries[1, at, :] = jnp.where(first, 0, scaled).astype(BF16)
    if pair:
        ones = jnp.where(row_ids((TALL - 128, rows)) == 0, 1.0, 0.0).astype(BF16)
        for n, ref in enumerate(kvs):
            keys[n] = ref[:, :128]
            turned[n, :128, :] = jnp.transpose(ref[:, 128:])
            turned[n, 128:, :] = ones
    row_max[...] = jnp.full_like(row_max, NEGATIVE)
    weighted[...] = jnp.zeros_like(weighted)

    def score(n, out):
        for m in range(2):
            out[m] = dot(keys[n], queries[m], NT)

    def soft_gather(slot, n, source, limit=None):
        for m in range(2):
            i = 2 * slot + m
            got = source[m]
            if limit is not None:
                got = jnp.where(row_ids((rows, wide)) <= limit, got, NEGATIVE)
            old = row_max[i, :1, :]
            new = jnp.maximum(old, jnp.max(got, axis=0, keepdims=True))
            soft = jnp.exp(got - new).astype(BF16)
            row_max[i] = jnp.broadcast_to(new, (8, wide))
            weighted[i] = weighted[i] * jnp.exp(old - new) + dot(turned[n], soft)

    def put(at, n, slot):
        units[0, at] = n
        units[1, at] = slot

    total = jnp.int32(0)
    for n in range(1, 8):
        put(total, n, 0)
        total = total + (blocks_at[n] < my_z).astype(jnp.int32)
    for extra in range(3):
        put(total + extra, 0, 1)

    column = lane_ids((1, wide))
    within = jnp.where(column < rows, column, column - rows)
    x_of = jnp.where(column < rows, lines_at[2 * pair], lines_at[2 * pair + 1])
    limit = jnp.where(x_of > my_x, rows, jnp.where(x_of == my_x, within, -1))
    score(0, scores[1])
    score(units[0, 0], scores[0])
    soft_gather(0, 0, scores[1], limit)

    def step(at, now, other):
        score(units[0, at + 1], scores[other])
        soft_gather(units[1, at], units[0, at], scores[now])

    def two(t, carry):
        step(2 * t, 0, 1)
        step(2 * t + 1, 1, 0)
        return carry

    lax.fori_loop(0, (total + 1) // 2, two, 0)

    for n, out in enumerate(outs):
        at = slice(n * rows, (n + 1) * rows)
        for m in range(2):
            top = row_max[m, :1, at]
            some = top > 0.5 * NEGATIVE
            row_sum = jnp.where(some, weighted[m, 128:129, at], 1.0)
            share = jnp.where(some, 1.0 / row_sum, 0.0)
            out[m, :128, :] = (weighted[m, :128, at] * share).astype(BF16)
            logs = jnp.where(some, top + jnp.log(row_sum), NEGATIVE)
            high = logs.astype(BF16).astype(F32)
            middle = (logs - high).astype(BF16).astype(F32)
            low = logs - high - middle
            tail = [high, middle, low, jnp.zeros((TALL - 131, rows), F32)]
            out[m, 128:, :] = jnp.concatenate(tail, axis=0).astype(BF16)


def finish_kernel(
    lambda_ref, p0, p1, p2, p3, read_ref, local_ref, window_ref, near_ref, before_ref, wr_ref, wa_ref,
    mine_out, other_out, logs_out,
):
    rows = read_ref.shape[0]
    parts = (p0, p1, p2, p3)
    maps = []
    for m in range(2):
        logs = []
        for p in parts:
            tail = p[m, 128:, :].astype(F32)
            logs.append(tail[:1] + tail[1:2] + tail[2:3])
        top = functools.reduce(jnp.maximum, logs)
        shares = [jnp.exp(a - top) for a in logs]
        total = functools.reduce(jnp.add, shares)
        logs_out[m : m + 1, :] = top + jnp.log(total)
        got = None
        for p, share in zip(parts, shares):
            term = p[m, :128, :].astype(F32) * (share / total)
            got = term if got is None else got + term
        maps.append(got)
    head = maps[0] - lambda_ref[...] * maps[1]
    head = head * lax.rsqrt(jnp.mean(head * head, axis=0, keepdims=True) + HEAD_EPS)
    att_mix = jnp.transpose(head.astype(BF16))
    state = state_before(window_ref[...], near_ref[...], before_ref[...])
    recurrent = local_ref[...] + exact(read_ref[...], state, NT)
    recurrent = pltpu.roll(recurrent, HD, 1)
    first = lane_ids((rows, 128)) < HD

    def per_head(values):
        low = jnp.sum(jnp.where(first, values, 0.0), axis=-1, keepdims=True)
        high = jnp.sum(jnp.where(first, 0.0, values), axis=-1, keepdims=True)
        return jnp.where(first, low, high) / HD

    centered = recurrent - per_head(recurrent)
    rec_mix = (centered * lax.rsqrt(per_head(centered * centered) + GROUP_EPS)).astype(BF16)
    mix = jnp.concatenate([rec_mix, att_mix], axis=1)
    core, y = lax.axis_index("c"), lax.axis_index("y")
    for n in range(8):
        at = slice(256 * n, 256 * n + 256)
        weight = jnp.concatenate([wr_ref[:, at], wa_ref[:, at]], axis=0)
        got = dot(mix, weight).astype(BF16)
        for place in range(4):
            even = got[96 * place : 96 * place + 48]
            odd = got[96 * place + 48 : 96 * place + 96]
            mine_out[(place - y) & 3, :, at] = jnp.where(core == 0, even, odd)
            other_out[(place - y) & 3, :, at] = jnp.where(core == 0, odd, even)


def pair_kernel(mine_ref, other_ref, *outs):
    for n, out in enumerate(outs):
        total = mine_ref[n].astype(F32) + other_ref[n].astype(F32)
        out[...] = total.astype(out.dtype)


def norm_kernel(own_ref, p1, p2, p3, gain_ref, out_ref):
    total = own_ref[...]
    for part in (p1, p2, p3):
        total = total + part[...].astype(F32)
    scale = lax.rsqrt(jnp.mean(total * total, axis=-1, keepdims=True) + NORM_EPS)
    out_ref[...] = (total * scale * gain_ref[...]).astype(BF16)


def per_device(
    hidden_in, in_gain, receptance_weight, key_weight, value_weight, decay_down, decay_up,
    decay_base, decay_shift, learn_rate, query_pair, key_pair, value_pair, mix_lambda,
    out_recurrent, out_attention, out_gain,
):
    permute = lax.ppermute
    together = lax.optimization_barrier
    rows = hidden_in.shape[0]
    half = rows // 2
    count = rows // SPAN
    shaped = jax.ShapeDtypeStruct

    up = permute(hidden_in, "y", ring(4, 1))
    down = permute(hidden_in, "y", ring(4, -1))
    mine = [up, down, permute(hidden_in, "y", ring(4, 2))]
    theirs = [permute(a, "c", ring(2, 1)) for a in (hidden_in, *mine)]
    turned_in = jnp.concatenate([hidden_in[half:], hidden_in[:half]], axis=0)
    pair_weights = jnp.concatenate([key_pair, value_pair, query_pair], axis=2).reshape(2048, 384)
    normed, q, kv = call(
        project_kernel,
        (shaped((rows, 2048), BF16), shaped((rows, 128), BF16), shaped((rows, 256), BF16)),
        (),
        (turned_in, *mine, *theirs, in_gain.reshape(8, 256), pair_weights),
        flops=2 * rows * 2048 * 896,
        name="project",
    )

    right = permute(kv, "z", ring(8, 1))
    left = permute(kv, "z", ring(8, -1))
    tile = (2 * count, SPAN, 128)
    chunked = call(
        chunk_kernel,
        (
            shaped(tile, F32), shaped(tile, F32), shaped(tile, F32), shaped((count, SPAN, 128), F32),
            shaped((count, SPAN, 128), F32), shaped((count, 128, 128), F32), shaped((count, 8, 128), F32),
        ),
        (),
        (
            normed, receptance_weight, key_weight, value_weight, decay_down, decay_up,
            decay_base.reshape(1, 128), decay_shift, learn_rate.reshape(1, 128),
        ),
        flops=6 * 10**9,
        name="chunks",
    )
    right1, left1, chunked, q = together((right, left, chunked, q))
    right = permute(right1, "z", ring(8, 1))
    left = permute(left1, "z", ring(8, -1))
    read, local, message = call(
        recurrent_kernel,
        (shaped((rows, 128), F32), shaped((rows, 128), F32), shaped((rows + 128, 128), BF16)),
        (),
        (*chunked, q),
        flops=6 * 10**9,
        name="recurrent",
    )
    right2, left2, message = together((right, left, message))
    right = permute(right2, "z", ring(8, 1))
    left = permute(left2, "z", ring(8, -1))
    messages = [
        message,
        permute(message, "x", ring(4, 1)),
        permute(message, "x", ring(4, -1)),
        permute(message, "x", ring(4, 2)),
    ]
    right3, left3, messages = together((right, left, messages))
    right4 = permute(right3, "z", ring(8, 1))
    before, line = call(
        along_x_kernel,
        (shaped((128, 128), F32), shaped((128, 128), BF16)),
        (), messages, scratch=(pltpu.VMEM((4, 128, 128), BF16),), flops=10**8, name="along_x",
    )
    lines = [permute(line, "z", ring(8, s)) for s in (1, 2, 3)]

    payload = shaped((2, TALL, rows), BF16)
    wide = 2 * rows

    def attend(pair, lead, arrays):
        return call(
            functools.partial(attention_kernel, pair),
            (payload,) * 2
            + ((shaped((8, rows, 128), BF16), shaped((8, TALL, rows), BF16)) if pair else ()),
            (),
            (*lead, *arrays),
            scratch=[
                pltpu.VMEM((4, 8, wide), F32), pltpu.VMEM((4, TALL, wide), F32),
                pltpu.VMEM((2, wide, 128), BF16), [pltpu.VMEM((2, rows, wide), F32)] * 2,
                pltpu.SMEM((2, 16), jnp.int32),
            ],
            flops=8 * 10**9,
            name=f"attention{pair}",
        )

    to_next, to_far, keys, turned = attend(
        1, messages[2:], (kv, right1, left1, right2, left2, right3, left3, right4)
    )
    to_next, to_far, keys, turned, line, lines = together((to_next, to_far, keys, turned, line, lines))
    from_before = permute(to_next, "x", ring(4, 1))
    from_far = permute(to_far, "x", ring(4, 2))
    window, near = call(
        window_kernel,
        (shaped((128, 128), BF16), shaped((128, 128), F32)),
        (), (line, *lines), flops=10**8, name="window",
    )
    window, keys = together((window, keys))
    window = permute(window, "z", ring(8, 4))
    ours, to_before = attend(0, messages[:2], (keys, turned))
    back = [ours, from_before, permute(to_before, "x", ring(4, -1)), from_far]
    ours, others, log_sums = call(
        finish_kernel,
        (shaped((4, rows // 8, 2048), BF16), shaped((4, rows // 8, 2048), BF16), shaped((2, rows), F32)),
        (),
        (mix_lambda.reshape(1, 1), *back, read, local, window, near, before, out_recurrent, out_attention),
        flops=10**9,
        name="finish",
    )
    theirs = permute(others, "c", ring(2, 1))
    piece = (rows // 8, 2048)
    own, plus1, plus2, plus3 = call(
        pair_kernel,
        (shaped(piece, F32),) + (shaped(piece, BF16),) * 3,
        (), (ours, theirs), flops=10**8, name="pair",
    )
    layer_out = call(
        norm_kernel,
        shaped(piece, BF16),
        (),
        (
            own,
            permute(plus1, "y", ring(4, 1)),
            permute(plus3, "y", ring(4, -1)),
            permute(plus2, "y", ring(4, 2)),
            out_gain.reshape(1, 2048),
        ),
        flops=10**8,
        name="norm",
    )
    return (layer_out, log_sums[None])


def solution(mesh):
    split = Mesh(mesh.devices.reshape(8, 4, 4, 2), ("z", "x", "y", "c"))
    sp, tp = ("z", "x"), ("y", "c")
    placed = (
        P(sp, tp), P(), P(None, tp), P(None, tp), P(None, tp), P(), P(None, tp), P(tp), P(sp, tp),
        P(tp), P(None, tp, None), P(None, tp, None), P(None, tp, None), P(tp), P(tp, None),
        P(tp, None), P(),
    )
    return jax.shard_map(
        per_device,
        mesh=split,
        in_specs=placed,
        out_specs=(P(("z", "x", "y", "c"), None), P(tp, None, sp)),
        check_vma=False,
    )
```

```python
import functools
import math

import jax
import jax.numpy as jnp
from jax import lax
from jax.experimental import pallas as pl
from jax.experimental.pallas import tpu as pltpu
from jax.sharding import Mesh
from jax.sharding import PartitionSpec as P


HD = 64
F32 = jnp.float32
BF16 = jnp.bfloat16
DECAY_SCALE = math.exp(-0.5)
NORM_EPS = 1e-06
GROUP_EPS = 0.00064
HEAD_EPS = 1e-05
KEY_EPS = 1e-06
NEGATIVE = -1e30
SPAN = 64
MIB = 1024 * 1024
GRANT = 28
NT = (((1,), (1,)), ((), ()))
TN = (((0,), (0,)), ((), ()))
NN = (((1,), (0,)), ((), ()))


def call(kernel, outs, scalars, arrays, scratch=(), flops=0, grant=GRANT):
    return pl.pallas_call(
        kernel,
        out_shape=outs,
        in_specs=[pl.BlockSpec(memory_space=pltpu.SMEM)] * len(scalars)
        + [pl.BlockSpec(memory_space=pltpu.VMEM)] * len(arrays),
        out_specs=jax.tree.map(lambda _: pl.BlockSpec(memory_space=pltpu.VMEM), outs),
        scratch_shapes=list(scratch),
        compiler_params=pltpu.CompilerParams(vmem_limit_bytes=grant * MIB),
        cost_estimate=pl.CostEstimate(flops=flops, bytes_accessed=flops // 1000, transcendentals=0),
    )(*scalars, *arrays)


def dot(left, right, dims=NN):
    return lax.dot_general(left, right, dims, preferred_element_type=F32)


def halves(value):
    if value.dtype == BF16:
        return (value,)
    high = value.astype(BF16)
    return (high, (value - high.astype(F32)).astype(BF16))


def exact(left, right, dims=NN):
    left, right = halves(left), halves(right)
    total = dot(left[0], right[0], dims)
    for more in left[1:]:
        total = total + dot(more, right[0], dims)
    for more in right[1:]:
        total = total + dot(left[0], more, dims)
    return total


def ring(size, shift):
    return [(i, (i + shift) % size) for i in range(size)]


def lane_ids(shape):
    return lax.broadcasted_iota(jnp.int32, shape, len(shape) - 1)


def row_ids(shape):
    return lax.broadcasted_iota(jnp.int32, shape, len(shape) - 2)


def project_kernel(
    own, h1, h2, h3, g0, g1, g2, g3, gain_ref, weights,
    normed, q_out, kv_out,
):
    half = own.shape[0] // 2
    pieces = [
        h1[...], h2[...], h3[...],
        g0[...], g1[...], g2[...], g3[...],
        jnp.concatenate([own[half:], own[:half]], axis=0),
    ]
    squares = None
    for piece in pieces:
        wide = piece.astype(F32)
        part = wide * wide
        part = part[:, :128] + part[:, 128:]
        squares = part if squares is None else squares + part
    scale = lax.rsqrt(jnp.sum(squares, axis=-1, keepdims=True) / 2048.0 + NORM_EPS)
    y, core = lax.axis_index("y"), lax.axis_index("c")
    ys = [(y + 3) & 3, (y + 1) & 3, (y + 2) & 3]
    places = [2 * a + core for a in ys] + [2 * a + 1 - core for a in (y, *ys)] + [2 * y + core]
    for place, piece in zip(places, pieces):
        gain = gain_ref[pl.ds(place, 1), :]
        value = (piece.astype(F32) * scale * gain).astype(BF16)
        normed[:, pl.ds(pl.multiple_of(place * 256, 256), 256)] = value
    kv_out[...] = dot(normed[...], weights[:, :256]).astype(BF16)
    q_out[...] = dot(normed[...], weights[:, 256:]).astype(BF16)


def line_places():
    x = lax.axis_index("x")
    return [x, (x + 3) & 3, (x + 1) & 3, (x + 2) & 3]


def ring_places():
    z = lax.axis_index("z")
    return [z] + [(z + 8 + s) & 7 for s in (-1, 1, -2, 2, -3, 3, 4)]


def same_head():
    return (row_ids((128, 128)) < HD) == (lane_ids((128, 128)) < HD)


def diagonal_mask():
    return row_ids((128, 128)) == lane_ids((128, 128))


def compose(earlier, later, same):
    zero = jnp.zeros_like(later)
    return exact(earlier, jnp.where(same, later, zero)) + jnp.where(same, zero, later).astype(F32)


def chunk_kernel(
    normed, wr, wk, wv, wd, up_ref, base_ref, shift_ref, rate_ref,
    lower_out, reading_out, rhs_out, turned_out, reads_out, ends_out, last_out,
):
    both = dot(normed[...], jnp.concatenate([wr[...], wk[...]], axis=1))
    all_reads = both[:, :128].astype(BF16)
    all_keys = both[:, 128:].astype(BF16)
    both = dot(normed[...], jnp.concatenate([wv[...], wd[...]], axis=1))
    all_values = both[:, :128].astype(BF16)
    low = jnp.tanh(both[:, 128:]).astype(BF16)
    pre = dot(low, up_ref[...]) + base_ref[...]
    all_decay = -DECAY_SCALE * jax.nn.sigmoid(pre) + shift_ref[...]
    rows = normed.shape[0]
    count = rows // SPAN
    ones_block = jnp.where(same_head(), 1.0, 0.0).astype(BF16)
    first = lane_ids((SPAN, 128)) < HD
    t_ids = row_ids((SPAN, 128))
    s_ids = lane_ids((SPAN, 128)) % HD
    strict = s_ids < t_ids
    causal = s_ids <= t_ids
    tri = jnp.where(row_ids((SPAN, SPAN)) >= lane_ids((SPAN, SPAN)), 1.0, 0.0).astype(BF16)
    keep = (first, jnp.logical_not(first))
    zero = jnp.zeros((SPAN, 128), F32)
    for c in range(count):
        at = slice(c * SPAN, (c + 1) * SPAN)
        decay = all_decay[at, :]
        running = exact(tri, decay)
        before = running - decay
        middle = running[SPAN // 2 - 1 : SPAN // 2, :]
        ending = running[SPAN - 1 : SPAN, :]
        keys = all_keys[at, :].astype(F32)
        reads = all_reads[at, :].astype(F32)
        values = all_values[at, :].astype(F32)
        unit_keys = keys * lax.rsqrt(exact(keys * keys, ones_block) + KEY_EPS)
        erasing = unit_keys * rate_ref[...]
        grow = jnp.exp(middle - running)
        against = -unit_keys * jnp.exp(before - middle)
        read_scaled = reads * jnp.exp(running - middle)
        right = jnp.concatenate([erasing * grow, keys * grow], axis=0)
        left = jnp.concatenate(
            [jnp.where(k, side, 0.0) for k in keep for side in (against, read_scaled)], axis=0
        )
        scores = exact(left, right, NT)
        turned = pltpu.roll(values, HD, 1)
        to_end = jnp.exp(ending - running)
        ends_out[c] = jnp.concatenate([erasing * to_end, keys * to_end], axis=0)
        start = -unit_keys * jnp.exp(before)
        reads_out[c] = reads * jnp.exp(running)
        last_out[c] = jnp.broadcast_to(jnp.exp(ending), (8, 128))
        turned_out[c] = turned
        for h in range(2):
            lower = jnp.where(strict, scores[128 * h : 128 * h + SPAN], 0.0)
            lower_out[2 * c + h] = lower
            reading_out[2 * c + h] = jnp.where(causal, scores[128 * h + SPAN : 128 * h + 128], 0.0)
            side_values = jnp.where(keep[h], 0.0, turned)
            rhs_out[2 * c + h] = jnp.where(keep[h], start, 0.0) + exact(
                lower, jnp.concatenate([zero, side_values], axis=0).astype(BF16)
            )


def recurrent_kernel(
    lower_ref, reading_ref, rhs_ref, turned_ref, reads_ref, ends_ref, last_ref, query_ref,
    read_out, local_out, message_out,
):
    count = turned_ref.shape[0]
    rows = count * SPAN
    same = same_head()
    diagonal = diagonal_mask()
    first = lane_ids((SPAN, 128)) < HD
    keep = (first, jnp.logical_not(first))
    units = range(2 * count)
    lowers = [lower_ref[n] for n in units]
    state = [[rhs_ref[n, 8 * b : 8 * b + 8] for b in range(SPAN // 8)] for n in units]
    half = SPAN // 2

    def substitute(start):
        for s in range(start, start + half - 1):
            for n in units:
                row = state[n][s // 8][s % 8 : s % 8 + 1]
                for b in range(s // 8 if s % 8 < 7 else s // 8 + 1, (start + half) // 8):
                    state[n][b] = state[n][b] + lowers[n][8 * b : 8 * b + 8, s : s + 1] * row

    substitute(0)
    rest = jnp.zeros((128 - half, 128), F32)
    for n in units:
        above = jnp.concatenate(state[n][: half // 8] + [rest], axis=0)
        more = exact(lowers[n][half:], above)
        for b in range(half // 8, SPAN // 8):
            state[n][b] = state[n][b] + more[8 * b - half : 8 * b - half + 8]
    substitute(half)
    solved = [jnp.concatenate(one, axis=0) for one in state]
    prefix = jnp.where(diagonal, 1.0, 0.0).astype(F32)
    for c in range(count):
        got, moved = [], []
        for h in range(2):
            side_values = jnp.where(keep[h], 0.0, turned_ref[c])
            both = jnp.concatenate([solved[2 * c + h], side_values], axis=0)
            got.append(exact(reading_ref[2 * c + h], both))
            moved.append(exact(both, ends_ref[c], TN))
        lanes = lane_ids((128, 128)) < HD
        step = jnp.where(lanes, moved[0], moved[1]) + jnp.where(diagonal, last_ref[c, :1], 0.0)
        read_state = jnp.where(first, got[0], got[1]) + reads_ref[c]
        local = jnp.where(first, got[1], got[0])
        at = slice(c * SPAN, (c + 1) * SPAN)
        read_out[at, :] = exact(read_state, jnp.where(same, prefix, 0.0), NT)
        local_out[at, :] = local + exact(read_state, jnp.where(same, 0.0, prefix), NT)
        prefix = compose(prefix, step, same)
    message_out[:rows, :] = query_ref[...]
    message_out[rows:, :] = prefix.astype(BF16)


def along_x_kernel(m0, m1, m2, m3, before_out, total_out, parts):
    rows = m0.shape[0] - 128
    same = same_head()
    identity = jnp.where(diagonal_mask(), 1.0, 0.0).astype(BF16)
    mine = lax.axis_index("x")
    for place, ref in zip(line_places(), (m0, m1, m2, m3)):
        parts[place] = ref[rows:, :]
    total = parts[0]
    for j in range(1, 4):
        total = compose(total, parts[j], same)
    total_out[...] = total.astype(BF16)
    before = jnp.where(mine > 0, parts[0], identity)
    for j in range(1, 3):
        before = compose(before, jnp.where(j < mine, parts[j], identity), same)
    before_out[...] = before


def window_kernel(line_ref, p1, p2, p3, window_out, near_out):
    same = same_head()
    identity = jnp.where(diagonal_mask(), 1.0, 0.0).astype(BF16)
    mine = lax.axis_index("z")
    near = jnp.where(mine >= 3, p3[...], identity)
    for far, part in ((2, p2), (1, p1)):
        near = compose(near, jnp.where(mine >= far, part[...], identity), same)
    near_out[...] = near
    window_out[...] = compose(near, line_ref[...], same).astype(BF16)


def state_before(window, near, before):
    same = same_head()
    identity = jnp.where(diagonal_mask(), 1.0, 0.0).astype(BF16)
    window = jnp.where(lax.axis_index("z") >= 4, window, identity)
    total = compose(compose(window, near, same), before, same)
    return jnp.where(same, 0.0, total)


TALL = 144


def attention_kernel(pair, *refs):
    lead, refs = refs[:2], refs[2:]
    taken = 8 if pair else 2
    kvs, refs = refs[:taken], refs[taken:]
    outs, refs = refs[:2], refs[2:]
    keys, turned = refs[:2] if pair else kvs
    row_max, weighted, queries, scores, units = refs[2:] if pair else refs
    rows = lead[0].shape[0] - 128
    wide = 2 * rows
    blocks_at, lines_at = ring_places(), line_places()
    my_z, my_x = blocks_at[0], lines_at[0]
    first = lane_ids((rows, 128)) < HD
    for n, ref in enumerate(lead):
        scaled = (ref[:rows, :].astype(F32) * (HD**-0.5)).astype(BF16)
        at = slice(n * rows, (n + 1) * rows)
        queries[0, at, :] = jnp.where(first, scaled, 0).astype(BF16)
        queries[1, at, :] = jnp.where(first, 0, scaled).astype(BF16)
    if pair:
        ones = jnp.where(row_ids((TALL - 128, rows)) == 0, 1.0, 0.0).astype(BF16)
        for n, ref in enumerate(kvs):
            keys[n] = ref[:, :128]
            turned[n, :128, :] = jnp.transpose(ref[:, 128:])
            turned[n, 128:, :] = ones
    row_max[...] = jnp.full_like(row_max, NEGATIVE)
    weighted[...] = jnp.zeros_like(weighted)

    def score(n, out):
        for m in range(2):
            out[m] = dot(keys[n], queries[m], NT)

    def soft_gather(slot, n, source, limit=None):
        for m in range(2):
            i = 2 * slot + m
            got = source[m]
            if limit is not None:
                got = jnp.where(row_ids((rows, wide)) <= limit, got, NEGATIVE)
            old = row_max[i, :1, :]
            new = jnp.maximum(old, jnp.max(got, axis=0, keepdims=True))
            soft = jnp.exp(got - new).astype(BF16)
            row_max[i] = jnp.broadcast_to(new, (8, wide))
            weighted[i] = weighted[i] * jnp.exp(old - new) + dot(turned[n], soft)

    def put(at, n, slot):
        units[0, at] = n
        units[1, at] = slot

    total = jnp.int32(0)
    for n in range(1, 8):
        put(total, n, 0)
        total = total + (blocks_at[n] < my_z).astype(jnp.int32)
    for extra in range(3):
        put(total + extra, 0, 1)

    column = lane_ids((1, wide))
    within = jnp.where(column < rows, column, column - rows)
    x_of = jnp.where(column < rows, lines_at[2 * pair], lines_at[2 * pair + 1])
    limit = jnp.where(x_of > my_x, rows, jnp.where(x_of == my_x, within, -1))
    score(0, scores[1])
    score(units[0, 0], scores[0])
    soft_gather(0, 0, scores[1], limit)

    def step(at, now, other):
        score(units[0, at + 1], scores[other])
        soft_gather(units[1, at], units[0, at], scores[now])

    def two(t, carry):
        step(2 * t, 0, 1)
        step(2 * t + 1, 1, 0)
        return carry

    lax.fori_loop(0, (total + 1) // 2, two, 0)

    for n, out in enumerate(outs):
        at = slice(n * rows, (n + 1) * rows)
        for m in range(2):
            top = row_max[m, :1, at]
            some = top > 0.5 * NEGATIVE
            row_sum = jnp.where(some, weighted[m, 128:129, at], 1.0)
            share = jnp.where(some, 1.0 / row_sum, 0.0)
            out[m, :128, :] = (weighted[m, :128, at] * share).astype(BF16)
            logs = jnp.where(some, top + jnp.log(row_sum), NEGATIVE)
            high = logs.astype(BF16).astype(F32)
            middle = (logs - high).astype(BF16).astype(F32)
            low = logs - high - middle
            tail = [high, middle, low, jnp.zeros((TALL - 131, rows), F32)]
            out[m, 128:, :] = jnp.concatenate(tail, axis=0).astype(BF16)


def finish_kernel(
    lambda_ref, p0, p1, p2, p3, read_ref, local_ref, window_ref, near_ref, before_ref, wr_ref, wa_ref,
    mine_out, other_out, logs_out,
):
    rows = read_ref.shape[0]
    parts = (p0, p1, p2, p3)
    maps = []
    for m in range(2):
        logs = []
        for p in parts:
            tail = p[m, 128:, :].astype(F32)
            logs.append(tail[:1] + tail[1:2] + tail[2:3])
        top = functools.reduce(jnp.maximum, logs)
        shares = [jnp.exp(a - top) for a in logs]
        total = functools.reduce(jnp.add, shares)
        logs_out[m : m + 1, :] = top + jnp.log(total)
        got = None
        for p, share in zip(parts, shares):
            term = p[m, :128, :].astype(F32) * (share / total)
            got = term if got is None else got + term
        maps.append(got)
    head = maps[0] - lambda_ref[...] * maps[1]
    head = head * lax.rsqrt(jnp.mean(head * head, axis=0, keepdims=True) + HEAD_EPS)
    att_mix = jnp.transpose(head.astype(BF16))
    state = state_before(window_ref[...], near_ref[...], before_ref[...])
    recurrent = local_ref[...] + exact(read_ref[...], state, NT)
    recurrent = pltpu.roll(recurrent, HD, 1)
    first = lane_ids((rows, 128)) < HD

    def per_head(values):
        low = jnp.sum(jnp.where(first, values, 0.0), axis=-1, keepdims=True)
        high = jnp.sum(jnp.where(first, 0.0, values), axis=-1, keepdims=True)
        return jnp.where(first, low, high) / HD

    centered = recurrent - per_head(recurrent)
    rec_mix = (centered * lax.rsqrt(per_head(centered * centered) + GROUP_EPS)).astype(BF16)
    mix = jnp.concatenate([rec_mix, att_mix], axis=1)
    core, y = lax.axis_index("c"), lax.axis_index("y")
    for n in range(8):
        at = slice(256 * n, 256 * n + 256)
        weight = jnp.concatenate([wr_ref[:, at], wa_ref[:, at]], axis=0)
        got = dot(mix, weight).astype(BF16)
        for place in range(4):
            even = got[96 * place : 96 * place + 48]
            odd = got[96 * place + 48 : 96 * place + 96]
            mine_out[(place - y) & 3, :, at] = jnp.where(core == 0, even, odd)
            other_out[(place - y) & 3, :, at] = jnp.where(core == 0, odd, even)


def pair_kernel(mine_ref, other_ref, *outs):
    for n, out in enumerate(outs):
        total = mine_ref[n].astype(F32) + other_ref[n].astype(F32)
        out[...] = total.astype(out.dtype)


def norm_kernel(own_ref, p1, p2, p3, gain_ref, out_ref):
    total = own_ref[...]
    for part in (p1, p2, p3):
        total = total + part[...].astype(F32)
    scale = lax.rsqrt(jnp.mean(total * total, axis=-1, keepdims=True) + NORM_EPS)
    out_ref[...] = (total * scale * gain_ref[...]).astype(BF16)


def per_device(
    hidden_in, in_gain, receptance_weight, key_weight, value_weight, decay_down, decay_up,
    decay_base, decay_shift, learn_rate, query_pair, key_pair, value_pair, mix_lambda,
    out_recurrent, out_attention, out_gain,
):
    permute = lax.ppermute
    together = lax.optimization_barrier
    rows = hidden_in.shape[0]
    half = rows // 2
    count = rows // SPAN
    shaped = jax.ShapeDtypeStruct

    up = permute(hidden_in, "y", ring(4, 1))
    down = permute(hidden_in, "y", ring(4, -1))
    mine = [up, down, permute(hidden_in, "y", ring(4, 2))]
    theirs = [permute(a, "c", ring(2, 1)) for a in (hidden_in, *mine)]
    turned_in = jnp.concatenate([hidden_in[half:], hidden_in[:half]], axis=0)
    pair_weights = jnp.concatenate([key_pair, value_pair, query_pair], axis=2).reshape(2048, 384)
    normed, q, kv = call(
        project_kernel,
        (shaped((rows, 2048), BF16), shaped((rows, 128), BF16), shaped((rows, 256), BF16)),
        (),
        (turned_in, *mine, *theirs, in_gain.reshape(8, 256), pair_weights),
        flops=2 * rows * 2048 * 896,
    )

    right = permute(kv, "z", ring(8, 1))
    left = permute(kv, "z", ring(8, -1))
    tile = (2 * count, SPAN, 128)
    chunked = call(
        chunk_kernel,
        (
            shaped(tile, F32), shaped(tile, F32), shaped(tile, F32), shaped((count, SPAN, 128), F32),
            shaped((count, SPAN, 128), F32), shaped((count, 128, 128), F32), shaped((count, 8, 128), F32),
        ),
        (),
        (
            normed, receptance_weight, key_weight, value_weight, decay_down, decay_up,
            decay_base.reshape(1, 128), decay_shift, learn_rate.reshape(1, 128),
        ),
        flops=6 * 10**9,
    )
    right1, left1, chunked, q = together((right, left, chunked, q))
    right = permute(right1, "z", ring(8, 1))
    left = permute(left1, "z", ring(8, -1))
    read, local, message = call(
        recurrent_kernel,
        (shaped((rows, 128), F32), shaped((rows, 128), F32), shaped((rows + 128, 128), BF16)),
        (),
        (*chunked, q),
        flops=6 * 10**9,
    )
    right2, left2, message = together((right, left, message))
    right = permute(right2, "z", ring(8, 1))
    left = permute(left2, "z", ring(8, -1))
    messages = [message]
    for shift in (1, -1, 2):
        messages.append(permute(message, "x", ring(4, shift)))
    right3, left3 = right, left
    right4 = permute(right3, "z", ring(8, 1))
    before, line = call(
        along_x_kernel,
        (shaped((128, 128), F32), shaped((128, 128), BF16)),
        (), messages, scratch=(pltpu.VMEM((4, 128, 128), BF16),), flops=10**8,
    )
    lines = [permute(line, "z", ring(8, s)) for s in (1, 2, 3)]

    payload = shaped((2, TALL, rows), BF16)
    wide = 2 * rows

    def attend(pair, lead, arrays):
        return call(
            functools.partial(attention_kernel, pair),
            (payload,) * 2
            + ((shaped((8, rows, 128), BF16), shaped((8, TALL, rows), BF16)) if pair else ()),
            (),
            (*lead, *arrays),
            scratch=[
                pltpu.VMEM((4, 8, wide), F32), pltpu.VMEM((4, TALL, wide), F32),
                pltpu.VMEM((2, wide, 128), BF16), [pltpu.VMEM((2, rows, wide), F32)] * 2,
                pltpu.SMEM((2, 16), jnp.int32),
            ],
            flops=8 * 10**9,
        )

    to_next, to_far, keys, turned = attend(
        1, messages[2:], (kv, right1, left1, right2, left2, right3, left3, right4)
    )
    to_next, to_far, keys, turned, line, lines = together((to_next, to_far, keys, turned, line, lines))
    from_before = permute(to_next, "x", ring(4, 1))
    from_far = permute(to_far, "x", ring(4, 2))
    window, near = call(
        window_kernel,
        (shaped((128, 128), BF16), shaped((128, 128), F32)),
        (), (line, *lines), flops=10**8,
    )
    window, keys = together((window, keys))
    window = permute(window, "z", ring(8, 4))
    ours, to_before = attend(0, messages[:2], (keys, turned))
    back = [ours, from_before, permute(to_before, "x", ring(4, -1)), from_far]
    ours, others, log_sums = call(
        finish_kernel,
        (shaped((4, rows // 8, 2048), BF16), shaped((4, rows // 8, 2048), BF16), shaped((2, rows), F32)),
        (),
        (mix_lambda.reshape(1, 1), *back, read, local, window, near, before, out_recurrent, out_attention),
        flops=10**9,
    )
    theirs = permute(others, "c", ring(2, 1))
    piece = (rows // 8, 2048)
    own, plus1, plus2, plus3 = call(
        pair_kernel,
        (shaped(piece, F32),) + (shaped(piece, BF16),) * 3,
        (), (ours, theirs), flops=10**8,
    )
    layer_out = call(
        norm_kernel,
        shaped(piece, BF16),
        (),
        (
            own,
            permute(plus1, "y", ring(4, 1)),
            permute(plus3, "y", ring(4, -1)),
            permute(plus2, "y", ring(4, 2)),
            out_gain.reshape(1, 2048),
        ),
        flops=10**8,
    )
    return (layer_out, log_sums[None])


def solution(mesh):
    split = Mesh(mesh.devices.reshape(8, 4, 4, 2), ("z", "x", "y", "c"))
    sp, tp = ("z", "x"), ("y", "c")
    placed = (
        P(sp, tp), P(), P(None, tp), P(None, tp), P(None, tp), P(), P(None, tp), P(tp), P(sp, tp),
        P(tp), P(None, tp, None), P(None, tp, None), P(None, tp, None), P(tp), P(tp, None),
        P(tp, None), P(),
    )
    return jax.shard_map(
        per_device,
        mesh=split,
        in_specs=placed,
        out_specs=(P(("z", "x", "y", "c"), None), P(tp, None, sp)),
        check_vma=False,
    )
```

```python
import functools
import math

import jax
import jax.numpy as jnp
from jax import lax
from jax.experimental import pallas as pl
from jax.experimental.pallas import tpu as pltpu
from jax.sharding import Mesh
from jax.sharding import PartitionSpec as P


HD = 64
F32 = jnp.float32
BF16 = jnp.bfloat16
DECAY_SCALE = math.exp(-0.5)
NORM_EPS = 1e-06
GROUP_EPS = 0.00064
HEAD_EPS = 1e-05
KEY_EPS = 1e-06
NEGATIVE = -1e30
SPAN = 64
MIB = 1024 * 1024
GRANT = 28
NT = (((1,), (1,)), ((), ()))
TN = (((0,), (0,)), ((), ()))
NN = (((1,), (0,)), ((), ()))


def call(kernel, outs, scalars, arrays, scratch=(), flops=0, grant=GRANT):
    return pl.pallas_call(
        kernel,
        out_shape=outs,
        in_specs=[pl.BlockSpec(memory_space=pltpu.SMEM)] * len(scalars)
        + [pl.BlockSpec(memory_space=pltpu.VMEM)] * len(arrays),
        out_specs=jax.tree.map(lambda _: pl.BlockSpec(memory_space=pltpu.VMEM), outs),
        scratch_shapes=list(scratch),
        compiler_params=pltpu.CompilerParams(vmem_limit_bytes=grant * MIB),
        cost_estimate=pl.CostEstimate(flops=flops, bytes_accessed=flops // 1000, transcendentals=0),
    )(*scalars, *arrays)


def dot(left, right, dims=NN):
    return lax.dot_general(left, right, dims, preferred_element_type=F32)


def halves(value):
    if value.dtype == BF16:
        return (value,)
    high = value.astype(BF16)
    return (high, (value - high.astype(F32)).astype(BF16))


def exact(left, right, dims=NN):
    left, right = halves(left), halves(right)
    total = dot(left[0], right[0], dims)
    for more in left[1:]:
        total = total + dot(more, right[0], dims)
    for more in right[1:]:
        total = total + dot(left[0], more, dims)
    return total


def ring(size, shift):
    return [(i, (i + shift) % size) for i in range(size)]


def lane_ids(shape):
    return lax.broadcasted_iota(jnp.int32, shape, len(shape) - 1)


def row_ids(shape):
    return lax.broadcasted_iota(jnp.int32, shape, len(shape) - 2)


def project_kernel(
    own, h1, h2, h3, g0, g1, g2, g3, gain_ref, weights,
    normed, q_out, kv_out,
):
    half = own.shape[0] // 2
    pieces = [
        h1[...], h2[...], h3[...],
        g0[...], g1[...], g2[...], g3[...],
        jnp.concatenate([own[half:], own[:half]], axis=0),
    ]
    squares = None
    for piece in pieces:
        wide = piece.astype(F32)
        part = wide * wide
        part = part[:, :128] + part[:, 128:]
        squares = part if squares is None else squares + part
    scale = lax.rsqrt(jnp.sum(squares, axis=-1, keepdims=True) / 2048.0 + NORM_EPS)
    y, core = lax.axis_index("y"), lax.axis_index("c")
    ys = [(y + 3) & 3, (y + 1) & 3, (y + 2) & 3]
    places = [2 * a + core for a in ys] + [2 * a + 1 - core for a in (y, *ys)] + [2 * y + core]
    for place, piece in zip(places, pieces):
        gain = gain_ref[pl.ds(place, 1), :]
        value = (piece.astype(F32) * scale * gain).astype(BF16)
        normed[:, pl.ds(pl.multiple_of(place * 256, 256), 256)] = value
    kv_out[...] = dot(normed[...], weights[:, :256]).astype(BF16)
    q_out[...] = dot(normed[...], weights[:, 256:]).astype(BF16)


def line_places():
    x = lax.axis_index("x")
    return [x, (x + 3) & 3, (x + 1) & 3, (x + 2) & 3]


def ring_places():
    z = lax.axis_index("z")
    return [z] + [(z + 8 + s) & 7 for s in (-1, 1, -2, 2, -3, 3, 4)]


def same_head():
    return (row_ids((128, 128)) < HD) == (lane_ids((128, 128)) < HD)


def diagonal_mask():
    return row_ids((128, 128)) == lane_ids((128, 128))


def compose(earlier, later, same):
    zero = jnp.zeros_like(later)
    return exact(earlier, jnp.where(same, later, zero)) + jnp.where(same, zero, later).astype(F32)


def chunk_kernel(
    normed, wr, wk, wv, wd, up_ref, base_ref, shift_ref, rate_ref,
    lower_out, reading_out, rhs_out, turned_out, reads_out, ends_out, last_out,
):
    both = dot(normed[...], jnp.concatenate([wr[...], wk[...]], axis=1))
    all_reads = both[:, :128].astype(BF16)
    all_keys = both[:, 128:].astype(BF16)
    both = dot(normed[...], jnp.concatenate([wv[...], wd[...]], axis=1))
    all_values = both[:, :128].astype(BF16)
    low = jnp.tanh(both[:, 128:]).astype(BF16)
    pre = dot(low, up_ref[...]) + base_ref[...]
    all_decay = -DECAY_SCALE * jax.nn.sigmoid(pre) + shift_ref[...]
    rows = normed.shape[0]
    count = rows // SPAN
    ones_block = jnp.where(same_head(), 1.0, 0.0).astype(BF16)
    first = lane_ids((SPAN, 128)) < HD
    t_ids = row_ids((SPAN, 128))
    s_ids = lane_ids((SPAN, 128)) % HD
    strict = s_ids < t_ids
    causal = s_ids <= t_ids
    tri = jnp.where(row_ids((SPAN, SPAN)) >= lane_ids((SPAN, SPAN)), 1.0, 0.0).astype(BF16)
    keep = (first, jnp.logical_not(first))
    zero = jnp.zeros((SPAN, 128), F32)
    for c in range(count):
        at = slice(c * SPAN, (c + 1) * SPAN)
        decay = all_decay[at, :]
        running = exact(tri, decay)
        before = running - decay
        middle = running[SPAN // 2 - 1 : SPAN // 2, :]
        ending = running[SPAN - 1 : SPAN, :]
        keys = all_keys[at, :].astype(F32)
        reads = all_reads[at, :].astype(F32)
        values = all_values[at, :].astype(F32)
        unit_keys = keys * lax.rsqrt(exact(keys * keys, ones_block) + KEY_EPS)
        erasing = unit_keys * rate_ref[...]
        grow = jnp.exp(middle - running)
        against = -unit_keys * jnp.exp(before - middle)
        read_scaled = reads * jnp.exp(running - middle)
        right = jnp.concatenate([erasing * grow, keys * grow], axis=0)
        left = jnp.concatenate(
            [jnp.where(k, side, 0.0) for k in keep for side in (against, read_scaled)], axis=0
        )
        scores = exact(left, right, NT)
        turned = pltpu.roll(values, HD, 1)
        to_end = jnp.exp(ending - running)
        ends_out[c] = jnp.concatenate([erasing * to_end, keys * to_end], axis=0)
        start = -unit_keys * jnp.exp(before)
        reads_out[c] = reads * jnp.exp(running)
        last_out[c] = jnp.broadcast_to(jnp.exp(ending), (8, 128))
        turned_out[c] = turned
        for h in range(2):
            lower = jnp.where(strict, scores[128 * h : 128 * h + SPAN], 0.0)
            lower_out[2 * c + h] = lower
            reading_out[2 * c + h] = jnp.where(causal, scores[128 * h + SPAN : 128 * h + 128], 0.0)
            side_values = jnp.where(keep[h], 0.0, turned)
            rhs_out[2 * c + h] = jnp.where(keep[h], start, 0.0) + exact(
                lower, jnp.concatenate([zero, side_values], axis=0).astype(BF16)
            )


def recurrent_kernel(
    lower_ref, reading_ref, rhs_ref, turned_ref, reads_ref, ends_ref, last_ref, query_ref,
    read_out, local_out, message_out,
):
    count = turned_ref.shape[0]
    rows = count * SPAN
    same = same_head()
    diagonal = diagonal_mask()
    first = lane_ids((SPAN, 128)) < HD
    keep = (first, jnp.logical_not(first))
    units = range(2 * count)
    lowers = [lower_ref[n] for n in units]
    state = [[rhs_ref[n, 8 * b : 8 * b + 8] for b in range(SPAN // 8)] for n in units]
    half = SPAN // 2

    def substitute(start):
        for s in range(start, start + half - 1):
            for n in units:
                row = state[n][s // 8][s % 8 : s % 8 + 1]
                for b in range(s // 8 if s % 8 < 7 else s // 8 + 1, (start + half) // 8):
                    state[n][b] = state[n][b] + lowers[n][8 * b : 8 * b + 8, s : s + 1] * row

    substitute(0)
    rest = jnp.zeros((128 - half, 128), F32)
    for n in units:
        above = jnp.concatenate(state[n][: half // 8] + [rest], axis=0)
        more = exact(lowers[n][half:], above)
        for b in range(half // 8, SPAN // 8):
            state[n][b] = state[n][b] + more[8 * b - half : 8 * b - half + 8]
    substitute(half)
    solved = [jnp.concatenate(one, axis=0) for one in state]
    prefix = jnp.where(diagonal, 1.0, 0.0).astype(F32)
    for c in range(count):
        got, moved = [], []
        for h in range(2):
            side_values = jnp.where(keep[h], 0.0, turned_ref[c])
            both = jnp.concatenate([solved[2 * c + h], side_values], axis=0)
            got.append(exact(reading_ref[2 * c + h], both))
            moved.append(exact(both, ends_ref[c], TN))
        lanes = lane_ids((128, 128)) < HD
        step = jnp.where(lanes, moved[0], moved[1]) + jnp.where(diagonal, last_ref[c, :1], 0.0)
        read_state = jnp.where(first, got[0], got[1]) + reads_ref[c]
        local = jnp.where(first, got[1], got[0])
        at = slice(c * SPAN, (c + 1) * SPAN)
        read_out[at, :] = exact(read_state, jnp.where(same, prefix, 0.0), NT)
        local_out[at, :] = local + exact(read_state, jnp.where(same, 0.0, prefix), NT)
        prefix = compose(prefix, step, same)
    message_out[:rows, :] = query_ref[...]
    message_out[rows:, :] = prefix.astype(BF16)


def along_x_kernel(m0, m1, m2, m3, before_out, total_out, parts):
    rows = m0.shape[0] - 128
    same = same_head()
    identity = jnp.where(diagonal_mask(), 1.0, 0.0).astype(BF16)
    mine = lax.axis_index("x")
    for place, ref in zip(line_places(), (m0, m1, m2, m3)):
        parts[place] = ref[rows:, :]
    total = parts[0]
    for j in range(1, 4):
        total = compose(total, parts[j], same)
    total_out[...] = total.astype(BF16)
    before = jnp.where(mine > 0, parts[0], identity)
    for j in range(1, 3):
        before = compose(before, jnp.where(j < mine, parts[j], identity), same)
    before_out[...] = before


def window_kernel(line_ref, p1, p2, p3, window_out, near_out):
    same = same_head()
    identity = jnp.where(diagonal_mask(), 1.0, 0.0).astype(BF16)
    mine = lax.axis_index("z")
    near = jnp.where(mine >= 3, p3[...], identity)
    for far, part in ((2, p2), (1, p1)):
        near = compose(near, jnp.where(mine >= far, part[...], identity), same)
    near_out[...] = near
    window_out[...] = compose(near, line_ref[...], same).astype(BF16)


def state_before(window, near, before):
    same = same_head()
    identity = jnp.where(diagonal_mask(), 1.0, 0.0).astype(BF16)
    window = jnp.where(lax.axis_index("z") >= 4, window, identity)
    total = compose(compose(window, near, same), before, same)
    return jnp.where(same, 0.0, total)


TALL = 144


def attention_kernel(others, *refs):
    many = 3 if others else 1
    lead, refs = refs[:many], refs[many:]
    taken = 8 if others else 2
    kvs, refs = refs[:taken], refs[taken:]
    outs, refs = refs[:many], refs[many:]
    keys, turned = refs[:2] if others else kvs
    row_max, weighted, queries, scores, units = refs[2:] if others else refs
    rows = lead[0].shape[0] - 128
    wide = many * rows
    blocks_at, lines_at = ring_places(), line_places()
    my_z, my_x = blocks_at[0], lines_at[0]
    first = lane_ids((rows, 128)) < HD
    for n, ref in enumerate(lead):
        scaled = (ref[:rows, :].astype(F32) * (HD**-0.5)).astype(BF16)
        at = slice(n * rows, (n + 1) * rows)
        queries[0, at, :] = jnp.where(first, scaled, 0).astype(BF16)
        queries[1, at, :] = jnp.where(first, 0, scaled).astype(BF16)
    if others:
        ones = jnp.where(row_ids((TALL - 128, rows)) == 0, 1.0, 0.0).astype(BF16)
        for n, ref in enumerate(kvs):
            keys[n] = ref[:, :128]
            turned[n, :128, :] = jnp.transpose(ref[:, 128:])
            turned[n, 128:, :] = ones

    def score(n, out):
        for m in range(2):
            out[m] = dot(keys[n], queries[m], NT)

    def soft_gather(n, source, limit=None):
        for m in range(2):
            got = source[m]
            if limit is None:
                old = row_max[m, :1, :]
                new = jnp.maximum(old, jnp.max(got, axis=0, keepdims=True))
            else:
                got = jnp.where(row_ids((rows, wide)) <= limit, got, NEGATIVE)
                new = jnp.max(got, axis=0, keepdims=True)
            soft = jnp.exp(got - new).astype(BF16)
            row_max[m] = jnp.broadcast_to(new, (8, wide))
            more = dot(turned[n], soft)
            weighted[m] = more if limit is not None else weighted[m] * jnp.exp(old - new) + more

    total = jnp.int32(0)
    units[0] = jnp.int32(0)
    for n in range(1, 8):
        units[total] = jnp.int32(n)
        total = total + (blocks_at[n] < my_z).astype(jnp.int32)
    units[total] = jnp.int32(0)

    column = lane_ids((1, wide))
    within, x_of = column, jnp.full((1, wide), lines_at[1 if others else 0])
    for n in range(1, many):
        within = jnp.where(column < n * rows, within, column - n * rows)
        x_of = jnp.where(column < n * rows, x_of, lines_at[1 + n])
    limit = jnp.where(x_of > my_x, rows, jnp.where(x_of == my_x, within, -1))
    score(0, scores[1])
    score(units[0], scores[0])
    soft_gather(0, scores[1], limit)

    def two(t, carry):
        score(units[2 * t + 1], scores[1])
        soft_gather(units[2 * t], scores[0])
        score(units[2 * t + 2], scores[0])
        soft_gather(units[2 * t + 1], scores[1])
        return carry

    lax.fori_loop(0, total // 2, two, 0)

    @pl.when(total % 2 == 1)
    def _():
        soft_gather(units[total - 1], scores[0])

    for n, out in enumerate(outs):
        at = slice(n * rows, (n + 1) * rows)
        for m in range(2):
            top = row_max[m, :1, at]
            some = top > 0.5 * NEGATIVE
            row_sum = jnp.where(some, weighted[m, 128:129, at], 1.0)
            share = jnp.where(some, 1.0 / row_sum, 0.0)
            out[m, :128, :] = (weighted[m, :128, at] * share).astype(BF16)
            logs = jnp.where(some, top + jnp.log(row_sum), NEGATIVE)
            high = logs.astype(BF16).astype(F32)
            middle = (logs - high).astype(BF16).astype(F32)
            low = logs - high - middle
            tail = [high, middle, low, jnp.zeros((TALL - 131, rows), F32)]
            out[m, 128:, :] = jnp.concatenate(tail, axis=0).astype(BF16)


def finish_kernel(
    lambda_ref, p0, p1, p2, p3, read_ref, local_ref, window_ref, near_ref, before_ref, wr_ref, wa_ref,
    mine_out, other_out, logs_out,
):
    rows = read_ref.shape[0]
    parts = (p0, p1, p2, p3)
    maps = []
    for m in range(2):
        logs = []
        for p in parts:
            tail = p[m, 128:, :].astype(F32)
            logs.append(tail[:1] + tail[1:2] + tail[2:3])
        top = functools.reduce(jnp.maximum, logs)
        shares = [jnp.exp(a - top) for a in logs]
        total = functools.reduce(jnp.add, shares)
        logs_out[m : m + 1, :] = top + jnp.log(total)
        got = None
        for p, share in zip(parts, shares):
            term = p[m, :128, :].astype(F32) * (share / total)
            got = term if got is None else got + term
        maps.append(got)
    head = maps[0] - lambda_ref[...] * maps[1]
    head = head * lax.rsqrt(jnp.mean(head * head, axis=0, keepdims=True) + HEAD_EPS)
    att_mix = jnp.transpose(head.astype(BF16))
    state = state_before(window_ref[...], near_ref[...], before_ref[...])
    recurrent = local_ref[...] + exact(read_ref[...], state, NT)
    recurrent = pltpu.roll(recurrent, HD, 1)
    first = lane_ids((rows, 128)) < HD

    def per_head(values):
        low = jnp.sum(jnp.where(first, values, 0.0), axis=-1, keepdims=True)
        high = jnp.sum(jnp.where(first, 0.0, values), axis=-1, keepdims=True)
        return jnp.where(first, low, high) / HD

    centered = recurrent - per_head(recurrent)
    rec_mix = (centered * lax.rsqrt(per_head(centered * centered) + GROUP_EPS)).astype(BF16)
    mix = jnp.concatenate([rec_mix, att_mix], axis=1)
    core, y = lax.axis_index("c"), lax.axis_index("y")
    for n in range(8):
        at = slice(256 * n, 256 * n + 256)
        weight = jnp.concatenate([wr_ref[:, at], wa_ref[:, at]], axis=0)
        got = dot(mix, weight).astype(BF16)
        for place in range(4):
            even = got[96 * place : 96 * place + 48]
            odd = got[96 * place + 48 : 96 * place + 96]
            mine_out[(place - y) & 3, :, at] = jnp.where(core == 0, even, odd)
            other_out[(place - y) & 3, :, at] = jnp.where(core == 0, odd, even)


def pair_kernel(mine_ref, other_ref, *outs):
    for n, out in enumerate(outs):
        total = mine_ref[n].astype(F32) + other_ref[n].astype(F32)
        out[...] = total.astype(out.dtype)


def norm_kernel(own_ref, p1, p2, p3, gain_ref, logs_ref, out_ref, logs_out):
    logs_out[...] = logs_ref[...]
    total = own_ref[...]
    for part in (p1, p2, p3):
        total = total + part[...].astype(F32)
    scale = lax.rsqrt(jnp.mean(total * total, axis=-1, keepdims=True) + NORM_EPS)
    out_ref[...] = (total * scale * gain_ref[...]).astype(BF16)


def per_device(
    hidden_in, in_gain, receptance_weight, key_weight, value_weight, decay_down, decay_up,
    decay_base, decay_shift, learn_rate, query_pair, key_pair, value_pair, mix_lambda,
    out_recurrent, out_attention, out_gain,
):
    permute = lax.ppermute
    together = lax.optimization_barrier
    rows = hidden_in.shape[0]
    half = rows // 2
    count = rows // SPAN
    shaped = jax.ShapeDtypeStruct

    up = permute(hidden_in, "y", ring(4, 1))
    down = permute(hidden_in, "y", ring(4, -1))
    mine = [up, down, permute(hidden_in, "y", ring(4, 2))]
    theirs = [permute(a, "c", ring(2, 1)) for a in (hidden_in, *mine)]
    turned_in = jnp.concatenate([hidden_in[half:], hidden_in[:half]], axis=0)
    pair_weights = jnp.concatenate([key_pair, value_pair, query_pair], axis=2).reshape(2048, 384)
    normed, q, kv = call(
        project_kernel,
        (shaped((rows, 2048), BF16), shaped((rows, 128), BF16), shaped((rows, 256), BF16)),
        (),
        (turned_in, *mine, *theirs, in_gain.reshape(8, 256), pair_weights),
        flops=2 * rows * 2048 * 896,
    )

    right = permute(kv, "z", ring(8, 1))
    left = permute(kv, "z", ring(8, -1))
    tile = (2 * count, SPAN, 128)
    chunked = call(
        chunk_kernel,
        (
            shaped(tile, F32), shaped(tile, F32), shaped(tile, F32), shaped((count, SPAN, 128), F32),
            shaped((count, SPAN, 128), F32), shaped((count, 128, 128), F32), shaped((count, 8, 128), F32),
        ),
        (),
        (
            normed, receptance_weight, key_weight, value_weight, decay_down, decay_up,
            decay_base.reshape(1, 128), decay_shift, learn_rate.reshape(1, 128),
        ),
        flops=6 * 10**9,
    )
    right1, left1, chunked, q = together((right, left, chunked, q))
    right = permute(right1, "z", ring(8, 1))
    left = permute(left1, "z", ring(8, -1))
    read, local, message = call(
        recurrent_kernel,
        (shaped((rows, 128), F32), shaped((rows, 128), F32), shaped((rows + 128, 128), BF16)),
        (),
        (*chunked, q),
        flops=6 * 10**9,
    )
    right2, left2, message = together((right, left, message))
    right = permute(right2, "z", ring(8, 1))
    left = permute(left2, "z", ring(8, -1))
    messages = [message]
    for shift in (1, -1, 2):
        messages.append(permute(message, "x", ring(4, shift)))
    right3, left3 = right, left
    right4 = permute(right3, "z", ring(8, 1))
    before, line = call(
        along_x_kernel,
        (shaped((128, 128), F32), shaped((128, 128), BF16)),
        (), messages, scratch=(pltpu.VMEM((4, 128, 128), BF16),), flops=10**8,
    )
    lines = [permute(line, "z", ring(8, s)) for s in (1, 2, 3)]

    payload = shaped((2, TALL, rows), BF16)

    def attend(others, lead, arrays):
        wide = len(lead) * rows
        return call(
            functools.partial(attention_kernel, others),
            (payload,) * len(lead)
            + ((shaped((8, rows, 128), BF16), shaped((8, TALL, rows), BF16)) if others else ()),
            (),
            (*lead, *arrays),
            scratch=[
                pltpu.VMEM((2, 8, wide), F32), pltpu.VMEM((2, TALL, wide), F32),
                pltpu.VMEM((2, wide, 128), BF16), [pltpu.VMEM((2, rows, wide), F32)] * 2,
                pltpu.SMEM((16,), jnp.int32),
            ],
            flops=8 * 10**9,
        )

    to_before, to_next, to_far, keys, turned = attend(
        True, messages[1:], (kv, right1, left1, right2, left2, right3, left3, right4)
    )
    to_before, to_next, to_far, keys, turned, line, lines = together(
        (to_before, to_next, to_far, keys, turned, line, lines)
    )
    from_far = permute(to_far, "x", ring(4, 2))
    from_before = permute(to_next, "x", ring(4, 1))
    from_next = permute(to_before, "x", ring(4, -1))
    window, near = call(
        window_kernel,
        (shaped((128, 128), BF16), shaped((128, 128), F32)),
        (), (line, *lines), flops=10**8,
    )
    window, keys = together((window, keys))
    window = permute(window, "z", ring(8, 4))
    (ours,) = attend(False, messages[:1], (keys, turned))
    back = [ours, from_before, from_next, from_far]
    ours, others, log_sums = call(
        finish_kernel,
        (shaped((4, rows // 8, 2048), BF16), shaped((4, rows // 8, 2048), BF16), shaped((2, rows), F32)),
        (),
        (mix_lambda.reshape(1, 1), *back, read, local, window, near, before, out_recurrent, out_attention),
        flops=10**9,
    )
    theirs = permute(others, "c", ring(2, 1))
    piece = (rows // 8, 2048)
    own, plus1, plus2, plus3 = call(
        pair_kernel,
        (shaped(piece, F32),) + (shaped(piece, BF16),) * 3,
        (), (ours, theirs), flops=10**8,
    )
    layer_out, log_sums = call(
        norm_kernel,
        (shaped(piece, BF16), shaped((2, rows), F32)),
        (),
        (
            own,
            permute(plus1, "y", ring(4, 1)),
            permute(plus3, "y", ring(4, -1)),
            permute(plus2, "y", ring(4, 2)),
            out_gain.reshape(1, 2048), log_sums,
        ),
        flops=10**8,
    )
    return (layer_out, log_sums[None])


def solution(mesh):
    split = Mesh(mesh.devices.reshape(8, 4, 4, 2), ("z", "x", "y", "c"))
    sp, tp = ("z", "x"), ("y", "c")
    placed = (
        P(sp, tp), P(), P(None, tp), P(None, tp), P(None, tp), P(), P(None, tp), P(tp), P(sp, tp),
        P(tp), P(None, tp, None), P(None, tp, None), P(None, tp, None), P(tp), P(tp, None),
        P(tp, None), P(),
    )
    return jax.shard_map(
        per_device,
        mesh=split,
        in_specs=placed,
        out_specs=(P(("z", "x", "y", "c"), None), P(tp, None, sp)),
        check_vma=False,
    )
```

```python
import functools
import math

import jax
import jax.numpy as jnp
from jax import lax
from jax.experimental import pallas as pl
from jax.experimental.pallas import tpu as pltpu
from jax.sharding import Mesh
from jax.sharding import PartitionSpec as P


HD = 64
F32 = jnp.float32
BF16 = jnp.bfloat16
DECAY_SCALE = math.exp(-0.5)
NORM_EPS = 1e-06
GROUP_EPS = 0.00064
HEAD_EPS = 1e-05
KEY_EPS = 1e-06
NEGATIVE = -1e30
SPAN = 64
MIB = 1024 * 1024
GRANT = 28
NT = (((1,), (1,)), ((), ()))
TN = (((0,), (0,)), ((), ()))
NN = (((1,), (0,)), ((), ()))


def call(kernel, outs, scalars, arrays, scratch=(), flops=0, grant=GRANT):
    return pl.pallas_call(
        kernel,
        out_shape=outs,
        in_specs=[pl.BlockSpec(memory_space=pltpu.SMEM)] * len(scalars)
        + [pl.BlockSpec(memory_space=pltpu.VMEM)] * len(arrays),
        out_specs=jax.tree.map(lambda _: pl.BlockSpec(memory_space=pltpu.VMEM), outs),
        scratch_shapes=list(scratch),
        compiler_params=pltpu.CompilerParams(vmem_limit_bytes=grant * MIB),
        cost_estimate=pl.CostEstimate(flops=flops, bytes_accessed=flops // 1000, transcendentals=0),
    )(*scalars, *arrays)


def dot(left, right, dims=NN):
    return lax.dot_general(left, right, dims, preferred_element_type=F32)


def halves(value):
    if value.dtype == BF16:
        return (value,)
    high = value.astype(BF16)
    return (high, (value - high.astype(F32)).astype(BF16))


def exact(left, right, dims=NN):
    left, right = halves(left), halves(right)
    total = dot(left[0], right[0], dims)
    for more in left[1:]:
        total = total + dot(more, right[0], dims)
    for more in right[1:]:
        total = total + dot(left[0], more, dims)
    return total


def ring(size, shift):
    return [(i, (i + shift) % size) for i in range(size)]


def lane_ids(shape):
    return lax.broadcasted_iota(jnp.int32, shape, len(shape) - 1)


def row_ids(shape):
    return lax.broadcasted_iota(jnp.int32, shape, len(shape) - 2)


def project_kernel(
    own, h1, h2, h3, h4, g0, g1, g2, g3, g4, gain_ref, weights,
    normed, q_out, kv_out,
):
    half = own.shape[0] // 2
    pieces = [
        h1[...], h2[...], jnp.concatenate([h3[...], h4[...]], axis=0),
        g0[...], g1[...], g2[...], jnp.concatenate([g3[...], g4[...]], axis=0),
        jnp.concatenate([own[half:], own[:half]], axis=0),
    ]
    squares = None
    for piece in pieces:
        wide = piece.astype(F32)
        part = wide * wide
        part = part[:, :128] + part[:, 128:]
        squares = part if squares is None else squares + part
    scale = lax.rsqrt(jnp.sum(squares, axis=-1, keepdims=True) / 2048.0 + NORM_EPS)
    y, core = lax.axis_index("y"), lax.axis_index("c")
    ys = [(y + 3) & 3, (y + 1) & 3, (y + 2) & 3]
    places = [2 * a + core for a in ys] + [2 * a + 1 - core for a in (y, *ys)] + [2 * y + core]
    for place, piece in zip(places, pieces):
        gain = gain_ref[pl.ds(place, 1), :]
        value = (piece.astype(F32) * scale * gain).astype(BF16)
        normed[:, pl.ds(pl.multiple_of(place * 256, 256), 256)] = value
    kv_out[...] = dot(normed[...], weights[:, :256]).astype(BF16)
    q_out[...] = dot(normed[...], weights[:, 256:]).astype(BF16)


def line_places():
    x = lax.axis_index("x")
    return [x, (x + 3) & 3, (x + 1) & 3, (x + 2) & 3]


def ring_places():
    z = lax.axis_index("z")
    return [z] + [(z + 8 + s) & 7 for s in (-1, 1, -2, 2, -3, 3, 4)]


def same_head():
    return (row_ids((128, 128)) < HD) == (lane_ids((128, 128)) < HD)


def diagonal_mask():
    return row_ids((128, 128)) == lane_ids((128, 128))


def compose(earlier, later, same):
    zero = jnp.zeros_like(later)
    return exact(earlier, jnp.where(same, later, zero)) + jnp.where(same, zero, later).astype(F32)


def chunk_kernel(
    normed, wr, wk, wv, wd, up_ref, base_ref, shift_ref, rate_ref,
    lower_out, reading_out, rhs_out, turned_out, reads_out, ends_out, last_out,
):
    both = dot(normed[...], jnp.concatenate([wr[...], wk[...]], axis=1))
    all_reads = both[:, :128].astype(BF16)
    all_keys = both[:, 128:].astype(BF16)
    both = dot(normed[...], jnp.concatenate([wv[...], wd[...]], axis=1))
    all_values = both[:, :128].astype(BF16)
    low = jnp.tanh(both[:, 128:]).astype(BF16)
    pre = dot(low, up_ref[...]) + base_ref[...]
    all_decay = -DECAY_SCALE * jax.nn.sigmoid(pre) + shift_ref[...]
    rows = normed.shape[0]
    count = rows // SPAN
    ones_block = jnp.where(same_head(), 1.0, 0.0).astype(BF16)
    first = lane_ids((SPAN, 128)) < HD
    t_ids = row_ids((SPAN, 128))
    s_ids = lane_ids((SPAN, 128)) % HD
    strict = s_ids < t_ids
    causal = s_ids <= t_ids
    tri = jnp.where(row_ids((SPAN, SPAN)) >= lane_ids((SPAN, SPAN)), 1.0, 0.0).astype(BF16)
    keep = (first, jnp.logical_not(first))
    zero = jnp.zeros((SPAN, 128), F32)
    for c in range(count):
        at = slice(c * SPAN, (c + 1) * SPAN)
        decay = all_decay[at, :]
        running = exact(tri, decay)
        before = running - decay
        middle = running[SPAN // 2 - 1 : SPAN // 2, :]
        ending = running[SPAN - 1 : SPAN, :]
        keys = all_keys[at, :].astype(F32)
        reads = all_reads[at, :].astype(F32)
        values = all_values[at, :].astype(F32)
        unit_keys = keys * lax.rsqrt(exact(keys * keys, ones_block) + KEY_EPS)
        erasing = unit_keys * rate_ref[...]
        grow = jnp.exp(middle - running)
        against = -unit_keys * jnp.exp(before - middle)
        read_scaled = reads * jnp.exp(running - middle)
        right = jnp.concatenate([erasing * grow, keys * grow], axis=0)
        left = jnp.concatenate(
            [jnp.where(k, side, 0.0) for k in keep for side in (against, read_scaled)], axis=0
        )
        scores = exact(left, right, NT)
        turned = pltpu.roll(values, HD, 1)
        to_end = jnp.exp(ending - running)
        ends_out[c] = jnp.concatenate([erasing * to_end, keys * to_end], axis=0)
        start = -unit_keys * jnp.exp(before)
        reads_out[c] = reads * jnp.exp(running)
        last_out[c] = jnp.broadcast_to(jnp.exp(ending), (8, 128))
        turned_out[c] = turned
        for h in range(2):
            lower = jnp.where(strict, scores[128 * h : 128 * h + SPAN], 0.0)
            lower_out[2 * c + h] = lower
            reading_out[2 * c + h] = jnp.where(causal, scores[128 * h + SPAN : 128 * h + 128], 0.0)
            side_values = jnp.where(keep[h], 0.0, turned)
            rhs_out[2 * c + h] = jnp.where(keep[h], start, 0.0) + exact(
                lower, jnp.concatenate([zero, side_values], axis=0).astype(BF16)
            )


def recurrent_kernel(
    lower_ref, reading_ref, rhs_ref, turned_ref, reads_ref, ends_ref, last_ref, query_ref,
    read_out, local_out, message_out,
):
    count = turned_ref.shape[0]
    rows = count * SPAN
    same = same_head()
    diagonal = diagonal_mask()
    first = lane_ids((SPAN, 128)) < HD
    keep = (first, jnp.logical_not(first))
    units = range(2 * count)
    lowers = [lower_ref[n] for n in units]
    state = [[rhs_ref[n, 8 * b : 8 * b + 8] for b in range(SPAN // 8)] for n in units]
    half = SPAN // 2

    def substitute(start):
        for s in range(start, start + half - 1):
            for n in units:
                row = state[n][s // 8][s % 8 : s % 8 + 1]
                for b in range(s // 8 if s % 8 < 7 else s // 8 + 1, (start + half) // 8):
                    state[n][b] = state[n][b] + lowers[n][8 * b : 8 * b + 8, s : s + 1] * row

    substitute(0)
    rest = jnp.zeros((128 - half, 128), F32)
    for n in units:
        above = jnp.concatenate(state[n][: half // 8] + [rest], axis=0)
        more = exact(lowers[n][half:], above)
        for b in range(half // 8, SPAN // 8):
            state[n][b] = state[n][b] + more[8 * b - half : 8 * b - half + 8]
    substitute(half)
    solved = [jnp.concatenate(one, axis=0) for one in state]
    prefix = jnp.where(diagonal, 1.0, 0.0).astype(F32)
    for c in range(count):
        got, moved = [], []
        for h in range(2):
            side_values = jnp.where(keep[h], 0.0, turned_ref[c])
            both = jnp.concatenate([solved[2 * c + h], side_values], axis=0)
            got.append(exact(reading_ref[2 * c + h], both))
            moved.append(exact(both, ends_ref[c], TN))
        lanes = lane_ids((128, 128)) < HD
        step = jnp.where(lanes, moved[0], moved[1]) + jnp.where(diagonal, last_ref[c, :1], 0.0)
        read_state = jnp.where(first, got[0], got[1]) + reads_ref[c]
        local = jnp.where(first, got[1], got[0])
        at = slice(c * SPAN, (c + 1) * SPAN)
        read_out[at, :] = exact(read_state, jnp.where(same, prefix, 0.0), NT)
        local_out[at, :] = local + exact(read_state, jnp.where(same, 0.0, prefix), NT)
        prefix = compose(prefix, step, same)
    message_out[:rows, :] = query_ref[...]
    message_out[rows:, :] = prefix.astype(BF16)


def along_x_kernel(m0, m1, m2, m3, before_out, total_out, parts):
    rows = m0.shape[0] - 128
    same = same_head()
    identity = jnp.where(diagonal_mask(), 1.0, 0.0).astype(BF16)
    mine = lax.axis_index("x")
    for place, ref in zip(line_places(), (m0, m1, m2, m3)):
        parts[place] = ref[rows:, :]
    total = parts[0]
    for j in range(1, 4):
        total = compose(total, parts[j], same)
    total_out[...] = total.astype(BF16)
    before = jnp.where(mine > 0, parts[0], identity)
    for j in range(1, 3):
        before = compose(before, jnp.where(j < mine, parts[j], identity), same)
    before_out[...] = before


def window_kernel(line_ref, p1, p2, p3, window_out, near_out):
    same = same_head()
    identity = jnp.where(diagonal_mask(), 1.0, 0.0).astype(BF16)
    mine = lax.axis_index("z")
    near = jnp.where(mine >= 3, p3[...], identity)
    for far, part in ((2, p2), (1, p1)):
        near = compose(near, jnp.where(mine >= far, part[...], identity), same)
    near_out[...] = near
    window_out[...] = compose(near, line_ref[...], same).astype(BF16)


def state_before(window, near, before):
    same = same_head()
    identity = jnp.where(diagonal_mask(), 1.0, 0.0).astype(BF16)
    window = jnp.where(lax.axis_index("z") >= 4, window, identity)
    total = compose(compose(window, near, same), before, same)
    return jnp.where(same, 0.0, total)


TALL = 144


def attention_kernel(others, *refs):
    many = 3 if others else 1
    lead, refs = refs[:many], refs[many:]
    taken = 8 if others else 2
    kvs, refs = refs[:taken], refs[taken:]
    outs, refs = refs[:many], refs[many:]
    keys, turned = refs[:2] if others else kvs
    row_max, weighted, queries, scores, units = refs[2:] if others else refs
    rows = lead[0].shape[0] - 128
    wide = many * rows
    blocks_at, lines_at = ring_places(), line_places()
    my_z, my_x = blocks_at[0], lines_at[0]
    first = lane_ids((rows, 128)) < HD
    for n, ref in enumerate(lead):
        scaled = (ref[:rows, :].astype(F32) * (HD**-0.5)).astype(BF16)
        at = slice(n * rows, (n + 1) * rows)
        queries[0, at, :] = jnp.where(first, scaled, 0).astype(BF16)
        queries[1, at, :] = jnp.where(first, 0, scaled).astype(BF16)
    if others:
        ones = jnp.where(row_ids((TALL - 128, rows)) == 0, 1.0, 0.0).astype(BF16)
        for n, ref in enumerate(kvs):
            keys[n] = ref[:, :128]
            turned[n, :128, :] = jnp.transpose(ref[:, 128:])
            turned[n, 128:, :] = ones

    def score(n, out):
        for m in range(2):
            out[m] = dot(keys[n], queries[m], NT)

    def soft_gather(n, source, limit=None):
        for m in range(2):
            got = source[m]
            if limit is None:
                old = row_max[m, :1, :]
                new = jnp.maximum(old, jnp.max(got, axis=0, keepdims=True))
            else:
                got = jnp.where(row_ids((rows, wide)) <= limit, got, NEGATIVE)
                new = jnp.max(got, axis=0, keepdims=True)
            soft = jnp.exp(got - new).astype(BF16)
            row_max[m] = jnp.broadcast_to(new, (8, wide))
            more = dot(turned[n], soft)
            weighted[m] = more if limit is not None else weighted[m] * jnp.exp(old - new) + more

    total = jnp.int32(0)
    units[0] = jnp.int32(0)
    for n in range(1, 8):
        units[total] = jnp.int32(n)
        total = total + (blocks_at[n] < my_z).astype(jnp.int32)
    units[total] = jnp.int32(0)

    column = lane_ids((1, wide))
    within, x_of = column, jnp.full((1, wide), lines_at[1 if others else 0])
    for n in range(1, many):
        within = jnp.where(column < n * rows, within, column - n * rows)
        x_of = jnp.where(column < n * rows, x_of, lines_at[1 + n])
    limit = jnp.where(x_of > my_x, rows, jnp.where(x_of == my_x, within, -1))
    score(0, scores[1])
    score(units[0], scores[0])
    soft_gather(0, scores[1], limit)

    def two(t, carry):
        score(units[2 * t + 1], scores[1])
        soft_gather(units[2 * t], scores[0])
        score(units[2 * t + 2], scores[0])
        soft_gather(units[2 * t + 1], scores[1])
        return carry

    lax.fori_loop(0, total // 2, two, 0)

    @pl.when(total % 2 == 1)
    def _():
        soft_gather(units[total - 1], scores[0])

    for n, out in enumerate(outs):
        at = slice(n * rows, (n + 1) * rows)
        for m in range(2):
            top = row_max[m, :1, at]
            some = top > 0.5 * NEGATIVE
            row_sum = jnp.where(some, weighted[m, 128:129, at], 1.0)
            share = jnp.where(some, 1.0 / row_sum, 0.0)
            out[m, :128, :] = (weighted[m, :128, at] * share).astype(BF16)
            logs = jnp.where(some, top + jnp.log(row_sum), NEGATIVE)
            high = logs.astype(BF16).astype(F32)
            middle = (logs - high).astype(BF16).astype(F32)
            low = logs - high - middle
            tail = [high, middle, low, jnp.zeros((TALL - 131, rows), F32)]
            out[m, 128:, :] = jnp.concatenate(tail, axis=0).astype(BF16)


def finish_kernel(
    lambda_ref, p0, p1, p2, p3, read_ref, local_ref, window_ref, near_ref, before_ref, wr_ref, wa_ref,
    mine_out, other_out, logs_out,
):
    rows = read_ref.shape[0]
    parts = (p0, p1, p2, p3)
    maps = []
    for m in range(2):
        logs = []
        for p in parts:
            tail = p[m, 128:, :].astype(F32)
            logs.append(tail[:1] + tail[1:2] + tail[2:3])
        top = functools.reduce(jnp.maximum, logs)
        shares = [jnp.exp(a - top) for a in logs]
        total = functools.reduce(jnp.add, shares)
        logs_out[m : m + 1, :] = top + jnp.log(total)
        got = None
        for p, share in zip(parts, shares):
            term = p[m, :128, :].astype(F32) * (share / total)
            got = term if got is None else got + term
        maps.append(got)
    head = maps[0] - lambda_ref[...] * maps[1]
    head = head * lax.rsqrt(jnp.mean(head * head, axis=0, keepdims=True) + HEAD_EPS)
    att_mix = jnp.transpose(head.astype(BF16))
    state = state_before(window_ref[...], near_ref[...], before_ref[...])
    recurrent = local_ref[...] + exact(read_ref[...], state, NT)
    recurrent = pltpu.roll(recurrent, HD, 1)
    first = lane_ids((rows, 128)) < HD

    def per_head(values):
        low = jnp.sum(jnp.where(first, values, 0.0), axis=-1, keepdims=True)
        high = jnp.sum(jnp.where(first, 0.0, values), axis=-1, keepdims=True)
        return jnp.where(first, low, high) / HD

    centered = recurrent - per_head(recurrent)
    rec_mix = (centered * lax.rsqrt(per_head(centered * centered) + GROUP_EPS)).astype(BF16)
    mix = jnp.concatenate([rec_mix, att_mix], axis=1)
    core, y = lax.axis_index("c"), lax.axis_index("y")
    for n in range(8):
        at = slice(256 * n, 256 * n + 256)
        weight = jnp.concatenate([wr_ref[:, at], wa_ref[:, at]], axis=0)
        got = dot(mix, weight).astype(BF16)
        for place in range(4):
            even = got[96 * place : 96 * place + 48]
            odd = got[96 * place + 48 : 96 * place + 96]
            mine_out[(place - y) & 3, :, at] = jnp.where(core == 0, even, odd)
            other_out[(place - y) & 3, :, at] = jnp.where(core == 0, odd, even)


def pair_kernel(mine_ref, other_ref, *outs):
    for n, out in enumerate(outs):
        total = mine_ref[n].astype(F32) + other_ref[n].astype(F32)
        out[...] = total.astype(out.dtype)


def norm_kernel(own_ref, p1, p2, p3, gain_ref, logs_ref, out_ref, logs_out):
    logs_out[...] = logs_ref[...]
    total = own_ref[...]
    for part in (p1, p2, p3):
        total = total + part[...].astype(F32)
    scale = lax.rsqrt(jnp.mean(total * total, axis=-1, keepdims=True) + NORM_EPS)
    out_ref[...] = (total * scale * gain_ref[...]).astype(BF16)


def per_device(
    hidden_in, in_gain, receptance_weight, key_weight, value_weight, decay_down, decay_up,
    decay_base, decay_shift, learn_rate, query_pair, key_pair, value_pair, mix_lambda,
    out_recurrent, out_attention, out_gain,
):
    permute = lax.ppermute
    together = lax.optimization_barrier
    rows = hidden_in.shape[0]
    half = rows // 2
    count = rows // SPAN
    shaped = jax.ShapeDtypeStruct

    up = permute(hidden_in, "y", ring(4, 1))
    down = permute(hidden_in, "y", ring(4, -1))
    mine = [
        up, down, permute(up[:half], "y", ring(4, 1)), permute(hidden_in[half:], "y", ring(4, 2)),
    ]
    theirs = [permute(a, "c", ring(2, 1)) for a in (hidden_in, *mine)]
    turned_in = jnp.concatenate([hidden_in[half:], hidden_in[:half]], axis=0)
    pair_weights = jnp.concatenate([key_pair, value_pair, query_pair], axis=2).reshape(2048, 384)
    normed, q, kv = call(
        project_kernel,
        (shaped((rows, 2048), BF16), shaped((rows, 128), BF16), shaped((rows, 256), BF16)),
        (),
        (turned_in, *mine, *theirs, in_gain.reshape(8, 256), pair_weights),
        flops=2 * rows * 2048 * 896,
    )

    right = permute(kv, "z", ring(8, 1))
    left = permute(kv, "z", ring(8, -1))
    tile = (2 * count, SPAN, 128)
    chunked = call(
        chunk_kernel,
        (
            shaped(tile, F32), shaped(tile, F32), shaped(tile, F32), shaped((count, SPAN, 128), F32),
            shaped((count, SPAN, 128), F32), shaped((count, 128, 128), F32), shaped((count, 8, 128), F32),
        ),
        (),
        (
            normed, receptance_weight, key_weight, value_weight, decay_down, decay_up,
            decay_base.reshape(1, 128), decay_shift, learn_rate.reshape(1, 128),
        ),
        flops=6 * 10**9,
    )
    right1, left1, chunked, q = together((right, left, chunked, q))
    right = permute(right1, "z", ring(8, 1))
    left = permute(left1, "z", ring(8, -1))
    read, local, message = call(
        recurrent_kernel,
        (shaped((rows, 128), F32), shaped((rows, 128), F32), shaped((rows + 128, 128), BF16)),
        (),
        (*chunked, q),
        flops=6 * 10**9,
    )
    right2, left2, message = together((right, left, message))
    right = permute(right2, "z", ring(8, 1))
    left = permute(left2, "z", ring(8, -1))
    messages = [message]
    for shift in (1, -1, 2):
        messages.append(permute(message, "x", ring(4, shift)))
    right3, left3 = right, left
    right4 = permute(right3, "z", ring(8, 1))
    before, line = call(
        along_x_kernel,
        (shaped((128, 128), F32), shaped((128, 128), BF16)),
        (), messages, scratch=(pltpu.VMEM((4, 128, 128), BF16),), flops=10**8,
    )
    lines = [permute(line, "z", ring(8, s)) for s in (1, 2, 3)]

    payload = shaped((2, TALL, rows), BF16)

    def attend(others, lead, arrays):
        wide = len(lead) * rows
        return call(
            functools.partial(attention_kernel, others),
            (payload,) * len(lead)
            + ((shaped((8, rows, 128), BF16), shaped((8, TALL, rows), BF16)) if others else ()),
            (),
            (*lead, *arrays),
            scratch=[
                pltpu.VMEM((2, 8, wide), F32), pltpu.VMEM((2, TALL, wide), F32),
                pltpu.VMEM((2, wide, 128), BF16), [pltpu.VMEM((2, rows, wide), F32)] * 2,
                pltpu.SMEM((16,), jnp.int32),
            ],
            flops=8 * 10**9,
        )

    to_before, to_next, to_far, keys, turned = attend(
        True, messages[1:], (kv, right1, left1, right2, left2, right3, left3, right4)
    )
    to_before, to_next, to_far, keys, turned, line, lines = together(
        (to_before, to_next, to_far, keys, turned, line, lines)
    )
    from_far = permute(to_far, "x", ring(4, 2))
    from_before = permute(to_next, "x", ring(4, 1))
    from_next = permute(to_before, "x", ring(4, -1))
    window, near = call(
        window_kernel,
        (shaped((128, 128), BF16), shaped((128, 128), F32)),
        (), (line, *lines), flops=10**8,
    )
    window, keys = together((window, keys))
    window = permute(window, "z", ring(8, 4))
    (ours,) = attend(False, messages[:1], (keys, turned))
    back = [ours, from_before, from_next, from_far]
    ours, others, log_sums = call(
        finish_kernel,
        (shaped((4, rows // 8, 2048), BF16), shaped((4, rows // 8, 2048), BF16), shaped((2, rows), F32)),
        (),
        (mix_lambda.reshape(1, 1), *back, read, local, window, near, before, out_recurrent, out_attention),
        flops=10**9,
    )
    theirs = permute(others, "c", ring(2, 1))
    piece = (rows // 8, 2048)
    own, plus1, plus2, plus3 = call(
        pair_kernel,
        (shaped(piece, F32),) + (shaped(piece, BF16),) * 3,
        (), (ours, theirs), flops=10**8,
    )
    layer_out, log_sums = call(
        norm_kernel,
        (shaped(piece, BF16), shaped((2, rows), F32)),
        (),
        (
            own,
            permute(plus1, "y", ring(4, 1)),
            permute(plus3, "y", ring(4, -1)),
            permute(plus2, "y", ring(4, 2)),
            out_gain.reshape(1, 2048), log_sums,
        ),
        flops=10**8,
    )
    return (layer_out, log_sums[None])


def solution(mesh):
    split = Mesh(mesh.devices.reshape(8, 4, 4, 2), ("z", "x", "y", "c"))
    sp, tp = ("z", "x"), ("y", "c")
    placed = (
        P(sp, tp), P(), P(None, tp), P(None, tp), P(None, tp), P(), P(None, tp), P(tp), P(sp, tp),
        P(tp), P(None, tp, None), P(None, tp, None), P(None, tp, None), P(tp), P(tp, None),
        P(tp, None), P(),
    )
    return jax.shard_map(
        per_device,
        mesh=split,
        in_specs=placed,
        out_specs=(P(("z", "x", "y", "c"), None), P(tp, None, sp)),
        check_vma=False,
    )
```
